256 devices in a mesh: ep: 64 (over z, y, core), tp: 4 (over x).
Axes of the slice: x: 4, y: 4, z: 8, core: 2. Of those that a mesh axis runs over, the one named last changes fastest.
Arguments:
- tokens: bfloat16 [16384, 1024], P('ep'), may hold values from -6 to 6
- cotangent: bfloat16 [16384, 1024], P('ep'), may hold values from -1.5 to 1.5
- routing: int32 [16384, 2], P('ep'), may hold values from 0 to 127, all different within a row; in each aligned block of 256 rows (0 to 255, 256 to 511, ...) at most 12 rows name the same one
- gate_weights: float32 [16384, 2], P('ep'), may hold values from 0.1 to 0.9
- gate_proj: bfloat16 [128, 1024, 512], P('ep', None, 'tp'), may hold values from -0.1875 to 0.1875
- up_proj: bfloat16 [128, 1024, 512], P('ep', None, 'tp'), may hold values from -0.1875 to 0.1875
- down_proj: bfloat16 [128, 512, 1024], P('ep', 'tp'), may hold values from -0.25 to 0.25
Outputs:
- tokens_grad: bfloat16 [16384, 1024], P('ep')
- gates_grad: float32 [16384, 2], P('ep')
- gate_proj_grad: float32 [128, 1024, 512], P('ep', None, 'tp')
- up_proj_grad: float32 [128, 1024, 512], P('ep', None, 'tp')
- down_proj_grad: float32 [128, 512, 1024], P('ep', 'tp')
The draws below stay inside these ranges and needn't reach their ends.
Inputs may be any that keep to these rules, and one draw needn't show every extreme that they name: `routing`: each row names 2 different experts; every expert is named by some row; within each aligned block of 256 rows (the tokens of one index of ep) no expert is named by more than 12 rows, a bound that some block reaches.
All inputs are finite; a program needn't handle non-finite values.
Results may differ from the reference program's by a relative error of at most 0.0015.
Values may be sent and summed in bfloat16 or wider, within the bound.
A program may use at most 128 MiB of HBM per device.

```python
import math
import jax
import jax.numpy as jnp
import numpy as np
from jax import lax

D = 1024
FF = 512
TOP = 2
TOK_DEV = 256
EXPERTS = 128
TOKENS = 16384
CAP = 12
N_EP = 64


def steps_of(own_key, shape, split, least, high):
    factor_of = 1.0
    for axis_at, parts in split:
        heights = jax.random.uniform(jax.random.fold_in(jax.random.fold_in(own_key, 6), axis_at), (parts,), jnp.float32, least / len(split), high / len(split))
        factor_of = factor_of * jnp.repeat(jnp.exp(heights), shape[axis_at] // parts).reshape((-1,) + (1,) * (len(shape) - 1 - axis_at))
    return factor_of


def shared_out(own_key, own, number, rows, number_of, top, reach, slope):
    sequence = jax.random.permutation(own_key, number_of)
    heavy_load, common = shares(number_of, rows * top, reach, slope, True), shares(number_of, rows * top, reach, slope, False)
    places = jnp.arange(number_of)

    def named(tallies, rotation):
        used = int((tallies > 0).sum())
        fixed = max(1, used // 4)
        moved = fixed + (places - fixed + rotation * (used - fixed)) % max(1, number_of - fixed)
        return jnp.zeros((number_of,), jnp.int32).at[sequence[jnp.where(places < fixed, places, moved)]].set(jnp.asarray(tallies, jnp.int32))

    tallies = jnp.where(number % 4 == 0, named(heavy_load, number // 4), named(common, number - number // 4 - 1))
    mixed = jax.random.permutation(jax.random.fold_in(own, 3), number_of)
    giver, sink = mixed[0:number_of // 2 * 2:2], mixed[1:number_of // 2 * 2:2]
    slack = jnp.minimum(tallies[giver] - 1, reach - tallies[sink]) // 2
    slack = jnp.where((giver == sequence[0]) | (sink == sequence[0]) | (tallies[sink] == 0), 0, jnp.maximum(slack, 0))
    moved = jax.random.randint(jax.random.fold_in(own, 4), (number_of // 2,), 0, 1 << 20) % (slack + 1)
    tallies = tallies.at[giver].add(-moved).at[sink].add(moved)
    labels = jnp.searchsorted(jnp.cumsum(tallies), jnp.arange(rows * top), side="right").astype(jnp.int32)
    listing = labels.reshape(top, rows).T
    listing = listing[jax.random.permutation(jax.random.fold_in(own, 1), rows)]
    rotation = jax.random.randint(jax.random.fold_in(own, 2), (rows, 1), 0, top)
    return jnp.take_along_axis(listing, (jnp.arange(top)[None, :] + rotation) % top, axis=1)


def shares(amount, total, limit, skew, full):
    portions = [(1 << 20) // math.isqrt(rank ** skew) + 1 for rank in range(1, amount + 1)]
    largest = limit if full else min(limit, max(-(-total // amount), total * portions[0] // sum(portions)))
    least = 1 if total - largest >= amount - 1 else 0
    counts, surplus = [largest] + [least] * (amount - 1), total - largest - least * (amount - 1)
    while surplus > 0:
        free = [i for i in range(1, amount) if counts[i] < largest] or [i for i in range(1, amount) if counts[i] < limit]
        pool, left = sum([portions[i] for i in free]), surplus
        for i in free:
            more = min(limit - counts[i], max(1, left * portions[i] // pool), surplus)
            counts[i] = counts[i] + more
            surplus = surplus - more
    return np.array(counts)


def gaussian(own_key, dims, scale, reach, shards=(), kind=jnp.bfloat16):
    loudness = steps_of(own_key, dims, shards, -0.22, 0.18) if shards else 1.0
    entries = jax.random.normal(own_key, dims, jnp.float32) * scale * loudness
    return jnp.minimum(jnp.maximum(entries, -reach), reach).astype(kind)


def setup_inputs(seed: int = 0) -> dict:
    streams_of = jax.random.split(jax.random.key(seed), 8)
    tokens = gaussian(streams_of[0], (TOKENS, D), 1.0, 6.0, ((0, 64),))
    cotangent = gaussian(streams_of[1], (TOKENS, D), 0.25, 1.5, ((0, 64),))
    routing_keys = jax.random.split(jax.random.fold_in(streams_of[2], 1), TOKENS // TOK_DEV)
    routing_turns = jax.random.permutation(jax.random.fold_in(streams_of[2], 3), TOKENS // TOK_DEV)
    routing = jax.vmap(lambda own, number: shared_out(jax.random.fold_in(streams_of[2], 2), own, number, TOK_DEV, EXPERTS, TOP, CAP, 2))(routing_keys, routing_turns).reshape((TOKENS, TOP))
    gate_weights = jnp.clip(0.1 + 0.79999997 * jax.random.uniform(streams_of[3], (TOKENS, TOP), jnp.float32) ** steps_of(streams_of[3], (TOKENS, TOP), ((0, 64),), -0.2, 0.2), 0.1, 0.9)
    gate_proj = gaussian(streams_of[4], (EXPERTS, D, FF), D ** -0.5, 0.1875, ((0, 64), (2, 4)))
    up_proj = gaussian(streams_of[5], (EXPERTS, D, FF), D ** -0.5, 0.1875, ((0, 64), (2, 4)))
    down_proj = gaussian(streams_of[6], (EXPERTS, FF, D), FF ** -0.5, 0.25, ((0, 64), (1, 4)))
    return dict(tokens=tokens, cotangent=cotangent, routing=routing, gate_weights=gate_weights, gate_proj=gate_proj, up_proj=up_proj, down_proj=down_proj)


def expert_pass(expert_rows, scaled, gate_matrix, up_matrix, down_matrix):
    gate_pre = jnp.dot(expert_rows, gate_matrix, preferred_element_type=jnp.float32).astype(jnp.bfloat16)
    up_pre = jnp.dot(expert_rows, up_matrix, preferred_element_type=jnp.float32).astype(jnp.bfloat16)
    gate_pre, up_pre = lax.optimization_barrier((gate_pre, up_pre))
    hidden_grad = jnp.dot(scaled, down_matrix.T, preferred_element_type=jnp.float32)
    gate_wide = gate_pre.astype(jnp.float32)
    up_wide = up_pre.astype(jnp.float32)
    sigmoid_gate = jax.nn.sigmoid(gate_wide)
    activated = gate_wide * sigmoid_gate
    hidden = activated * up_wide
    product = jnp.sum(hidden_grad * hidden, axis=-1)
    gate_pre_grad = (hidden_grad * up_wide * sigmoid_gate * (1.0 + gate_wide * (1.0 - sigmoid_gate))).astype(jnp.bfloat16)
    up_pre_grad = (hidden_grad * activated).astype(jnp.bfloat16)
    input_grad = jnp.dot(gate_pre_grad, gate_matrix.T, preferred_element_type=jnp.float32)
    input_grad = input_grad + jnp.dot(up_pre_grad, up_matrix.T, preferred_element_type=jnp.float32)
    down_grad = jnp.dot(hidden.astype(jnp.bfloat16).T, scaled, preferred_element_type=jnp.float32)
    gate_grad = jnp.dot(expert_rows.T, gate_pre_grad, preferred_element_type=jnp.float32)
    up_grad = jnp.dot(expert_rows.T, up_pre_grad, preferred_element_type=jnp.float32)
    return input_grad, product, gate_grad, up_grad, down_grad


def reference(tokens, cotangent, routing, gate_weights, gate_proj, up_proj, down_proj):
    pair_count = TOKENS * TOP
    row_limit = N_EP * CAP
    pair_expert = routing.reshape(pair_count)
    pair_weight = gate_weights.reshape(pair_count)

    def one_expert(expert_index):
        chosen = jnp.nonzero(pair_expert == expert_index, size=row_limit, fill_value=pair_count)[0].astype(jnp.int32)
        is_valid = chosen < pair_count
        safe_index = jnp.where(is_valid, chosen, 0).astype(jnp.int32)
        token_index = (safe_index // TOP).astype(jnp.int32)
        expert_rows = jnp.where(is_valid[:, None], tokens[token_index], jnp.zeros((), tokens.dtype))
        weight = jnp.where(is_valid, pair_weight[safe_index], jnp.zeros((), pair_weight.dtype))
        scaled = (weight[:, None] * cotangent[token_index].astype(jnp.float32)).astype(jnp.bfloat16)
        terms = expert_pass(expert_rows, scaled, gate_proj[expert_index], up_proj[expert_index], down_proj[expert_index])
        return (chosen,) + terms

    chosen, input_grad, product, gate_grad, up_grad, down_grad = lax.map(one_expert, jnp.arange(EXPERTS, dtype=jnp.int32))
    flat_chosen = chosen.reshape(-1)
    pair_grad = jnp.zeros((pair_count + 1, D), jnp.float32).at[flat_chosen].set(input_grad.reshape(-1, D))
    pair_product = jnp.zeros((pair_count + 1,), jnp.float32).at[flat_chosen].set(product.reshape(-1))
    tokens_grad = jnp.sum(pair_grad[:pair_count].reshape(TOKENS, TOP, D), axis=1).astype(jnp.bfloat16)
    gates_grad = (pair_product[:pair_count] / pair_weight).reshape(TOKENS, TOP)
    return tokens_grad, gates_grad, gate_grad, up_grad, down_grad
```

```python
import jax
import jax.numpy as jnp
from jax import lax
from jax.experimental import pallas as pl
from jax.experimental.pallas import tpu as pltpu
from jax.sharding import PartitionSpec as P

F32 = jnp.float32
BF16 = jnp.bfloat16
I32 = jnp.int32
MESH = pl.DeviceIdType.MESH

NZ, NY, NC, NX = 8, 4, 2, 4
PLANE = NY * NC
TOK = 256
D = 1024
Q = 256
FS = 128
CAP = 12
SLOT = 2 * CAP
ROWS = PLANE * SLOT
DENSE = TOK + 8
HALF = 128


def kernel(
    tok, cot, rt, gw, wg, wu, wd,
    tg_out, gg_out, dg_out, du_out, dd_out,
    bk, rb, sx, rx, xl, xr, wgu, wds, wq, sl, upper, ts, gu2, h2,
    gx, pr, prx, prs, prr, igs, igr, db, rm, rp, tq,
    z_s, z_r, rb_s, rb_r, ip_s, ip_r, x_s, x_r, w_s, w_r, g_s, g_r, gf_s, gf_r,
    p_s, p_r, pp_s, pp_r, ig_s, ig_r, c_s, c_r, t_s, t_r,
):
    e = lax.axis_index("ep")
    x = lax.axis_index("tp")
    z = e // PLANE
    y = (e % PLANE) // NC
    c = e % NC
    half = x % 2

    def at_z(step):
        return (((z + step) % NZ) * PLANE + y * NC + c, x)

    def at_plane(j, sign):
        dy, dc = j // NC, j % NC
        return (z * PLANE + ((y + sign * dy + NY) % NY) * NC + (c + dc) % NC, x)

    def at_x(step):
        return (e, (x + step) % NX)

    def remote(src, dst, ssem, rsem, dev):
        return pltpu.make_async_remote_copy(
            src_ref=src, dst_ref=dst, send_sem=ssem, recv_sem=rsem,
            device_id=dev, device_id_type=MESH,
        )

    def done(ref, sem):
        pltpu.make_async_copy(ref, ref, sem).wait()

    barrier = pltpu.get_barrier_semaphore()
    partners = [at_z(1), at_z(NZ - 1)]
    partners += [at_plane(j, 1) for j in range(1, PLANE)]
    partners += [at_x(s) for s in range(1, NX)]
    for dev in partners:
        pl.semaphore_signal(barrier, inc=1, device_id=dev, device_id_type=MESH)

    for k in range(2):
        cols = pl.ds(pl.multiple_of(half * 512 + k * Q, Q), Q)
        bk[0, k, 0] = tok[:, cols]
        bk[0, k, 1] = cot[:, cols]
    rb[0] = jnp.concatenate(
        [rt[...].astype(F32), gw[...], jnp.zeros((4, TOK), F32)], axis=0
    )
    for q in range(4):
        for i in range(2):
            wgu[q, :, i * FS:(i + 1) * FS] = wg[i, q * Q:(q + 1) * Q, :]
            wgu[q, :, 256 + i * FS:256 + (i + 1) * FS] = wu[i, q * Q:(q + 1) * Q, :]
            wds[q, i * FS:(i + 1) * FS, :] = wd[i, :, q * Q:(q + 1) * Q]
    upper[...] = (
        lax.broadcasted_iota(I32, (TOK, TOK), 0) < lax.broadcasted_iota(I32, (TOK, TOK), 1)
    ).astype(F32).astype(BF16)
    dg_out[...] = jnp.zeros_like(dg_out)
    du_out[...] = jnp.zeros_like(du_out)
    dd_out[...] = jnp.zeros_like(dd_out)

    pl.semaphore_wait(barrier, len(partners))

    def first_of(lanes):
        i = lax.broadcasted_iota(I32, (PLANE, SLOT, lanes), 1)
        return (i < CAP).reshape(ROWS, lanes)

    def lane_of_slot():
        i = lax.broadcasted_iota(I32, (PLANE, SLOT, FS), 1)
        l = lax.broadcasted_iota(I32, (PLANE, SLOT, FS), 2)
        return i == l

    def z_copies(dz):
        up = (dz + 1) % NZ
        down = (dz + NZ - 1) % NZ
        plus = [remote(bk.at[dz, h], bk.at[up, h], z_s.at[h, dz], z_r.at[h, up], at_z(1)) for h in range(2)]
        minus = [
            remote(bk.at[dz, h], bk.at[down, h], z_s.at[2 + h, dz], z_r.at[h, down], at_z(NZ - 1))
            for h in range(2)
        ]
        rplus = remote(rb.at[dz], rb.at[up], rb_s.at[0, dz], rb_r.at[up], at_z(1))
        rminus = remote(rb.at[dz], rb.at[down], rb_s.at[1, dz], rb_r.at[down], at_z(NZ - 1))
        return plus, minus, rplus, rminus

    def z_forward(dz):
        plus, minus, rplus, rminus = z_copies(dz)

        @pl.when(dz <= 3)
        def _():
            rplus.start()
            plus[0].start()

        @pl.when((dz == 0) | (dz >= 6))
        def _():
            rminus.start()

        @pl.when((dz == 0) | (dz >= 5))
        def _():
            minus[1].start()

        @pl.when(dz <= 2)
        def _():
            plus[1].start()

        @pl.when((dz == 0) | (dz >= 6))
        def _():
            minus[0].start()

    def z_wait(dz):
        done(rb.at[dz], rb_r.at[dz])
        for h in range(2):
            done(bk.at[dz, h], z_r.at[h, dz])

    def build(dz):
        e16 = lax.broadcasted_iota(I32, (16, TOK), 0)
        target = ((e16 // 4 - y) & 3) * NC + (((e16 // 2) - c) & 1)
        base = (target * SLOT + (e16 & 1) * CAP).astype(F32)
        block = rb[dz]
        chosen = block[0:2].astype(I32) - z * 16
        e0 = (e16 == chosen[0:1]).astype(F32)
        e1 = (e16 == chosen[1:2]).astype(F32)
        both = jnp.concatenate([e0, e1], axis=0).astype(BF16)
        before = jnp.dot(both, upper[...], preferred_element_type=F32)
        before0 = before[0:16]
        before1 = before[16:32] + jnp.sum(e0, axis=1, keepdims=True)
        s0 = jnp.sum(e0 * (base + before0 + 1.0), axis=0, keepdims=True) - 1.0
        s1 = jnp.sum(e1 * (base + before1 + 1.0), axis=0, keepdims=True) - 1.0
        slots = jnp.concatenate([s0, s1], axis=0).astype(I32)
        sl[dz, 0:2] = slots
        row = lax.broadcasted_iota(I32, (ROWS, TOK), 0)
        p0 = row == slots[0:1]
        p1 = row == slots[1:2]
        pick = (p0 | p1).astype(F32).astype(BF16)
        weight = jnp.sum(
            jnp.where(p0, block[2:3], 0.0) + jnp.where(p1, block[3:4], 0.0),
            axis=1, keepdims=True,
        )
        for h in range(2):
            t = jnp.dot(pick, bk[dz, h, 0], preferred_element_type=F32)
            s = jnp.dot(pick, bk[dz, h, 1], preferred_element_type=F32) * weight
            t = t.reshape(PLANE, 3, 8, Q).astype(BF16)
            s = s.reshape(PLANE, 3, 8, Q).astype(BF16)
            sx[dz, h, :, 0:3] = t
            sx[dz, h, :, 3:6] = s
            rx[dz, h, 0, 0:3] = t[0]
            rx[dz, h, 0, 3:6] = s[0]
        for j in range(1, PLANE):
            remote(
                sx.at[dz, :, j], rx.at[dz, :, j], ip_s.at[dz], ip_r.at[dz], at_plane(j, 1)
            ).start()

    def x_send(dz):
        done(rx.at[dz, :, pl.ds(1, PLANE - 1)], ip_r.at[dz])
        remote(rx.at[dz, 0], xl.at[dz], x_s.at[0, dz], x_r.at[0, dz], at_x(1)).start()
        remote(rx.at[dz, 1], xr.at[dz], x_s.at[1, dz], x_r.at[1, dz], at_x(NX - 1)).start()

    def quarter(k):
        return 2 * half + k if k < 2 else 2 * (1 - half) + (k - 2)

    def compute(dz):
        done(xl.at[dz], x_r.at[0, dz])
        done(xr.at[dz], x_r.at[1, dz])
        pre = jnp.zeros((ROWS, 512), F32)
        hg = jnp.zeros((ROWS, 256), F32)
        for k, src in enumerate((rx.at[dz, 0], rx.at[dz, 1], xl.at[dz], xr.at[dz])):
            t = src[:, 0:3].astype(F32).reshape(ROWS, Q).astype(BF16)
            s = src[:, 3:6].astype(F32).reshape(ROWS, Q).astype(BF16)
            ts[k, 0] = t
            ts[k, 1] = s
            pre = pre + jnp.dot(t, wgu[quarter(k)], preferred_element_type=F32)
            hg = hg + lax.dot_general(
                s, wds[quarter(k)], (((1,), (1,)), ((), ())), preferred_element_type=F32
            )
        first = first_of(FS)
        g = jnp.where(first, pre[:, 0:128], pre[:, 128:256]).astype(BF16).astype(F32)
        u = jnp.where(first, pre[:, 256:384], pre[:, 384:512]).astype(BF16).astype(F32)
        dh = jnp.where(first, hg[:, 0:128], hg[:, 128:256])
        sg = jax.nn.sigmoid(g)
        act = g * sg
        hidden = act * u
        product = jnp.sum(dh * hidden, axis=1, keepdims=True)
        placed = jnp.where(
            lane_of_slot(),
            jnp.broadcast_to(product, (ROWS, FS)).reshape(PLANE, SLOT, FS),
            0.0,
        )
        pr[dz] = jnp.sum(placed, axis=1)
        gg = dh * u * sg * (1.0 + g * (1.0 - sg))
        ug = dh * act
        gx[0, dz, :, 0:FS] = gg.astype(BF16)
        gx[0, dz, :, FS:2 * FS] = ug.astype(BF16)
        for i, v in enumerate((gg, ug, hidden)):
            lo = jnp.where(first, v, 0.0).astype(BF16)
            hi = jnp.where(first, 0.0, v).astype(BF16)
            if i < 2:
                gu2[:, 256 * i:256 * i + 128] = lo
                gu2[:, 256 * i + 128:256 * i + 256] = hi
            else:
                h2[:, 0:128] = lo
                h2[:, 128:256] = hi

    def weight_grads():
        for k in range(4):
            at = pl.ds(pl.multiple_of(quarter(k) * Q, Q), Q)
            o = lax.dot_general(
                ts[k, 0], gu2[...], (((0,), (0,)), ((), ())), preferred_element_type=F32
            )
            for i in range(2):
                dg_out[i, at, :] += o[:, i * FS:(i + 1) * FS]
                du_out[i, at, :] += o[:, 256 + i * FS:256 + (i + 1) * FS]
            o = lax.dot_general(
                h2[...], ts[k, 1], (((0,), (0,)), ((), ())), preferred_element_type=F32
            )
            for i in range(2):
                dd_out[i, :, at] += o[i * FS:(i + 1) * FS]

    z_forward(jnp.int32(0))
    for s in range(1, NX):
        remote(
            wgu.at[(x + s) % NX], wq.at[s - 1], w_s.at[s - 1], w_r.at[s - 1], at_x(s)
        ).start()
    build(jnp.int32(0))
    x_send(jnp.int32(0))

    def hop(k, carry):
        n = jnp.where(k < 4, 2, 1)

        def arrive(i, cc):
            dz = jnp.where(i == 0, k, NZ - k)
            z_wait(dz)
            z_forward(dz)
            return cc

        lax.fori_loop(0, n, arrive, 0)

        def make(i, cc):
            build(jnp.where(i == 0, k, NZ - k))
            return cc

        lax.fori_loop(0, n, make, 0)

        def work(i, cc):
            compute(jnp.where(i == 0, k - 1, NZ - k + 1))
            weight_grads()
            return cc

        lax.fori_loop(0, jnp.where(k > 1, 2, 1), work, 0)

        def pass_on(i, cc):
            x_send(jnp.where(i == 0, k, NZ - k))
            return cc

        lax.fori_loop(0, n, pass_on, 0)
        return carry

    lax.fori_loop(1, 5, hop, 0)
    compute(jnp.int32(4))

    def order(t):
        r = 7 - t
        return jnp.where(r % 2 == 1, (r + 1) // 2, (NZ - r // 2) % NZ)

    def g_start(t, cc):
        ch = order(t)
        remote(gx.at[0, ch], gx.at[1, ch], g_s.at[0, ch], g_r.at[0, ch], at_x(1)).start()
        remote(gx.at[0, ch], gx.at[2, ch], g_s.at[1, ch], g_r.at[1, ch], at_x(NX - 1)).start()
        return cc

    for s in range(1, NX):
        remote(pr, prx.at[s - 1], p_s.at[s - 1], p_r.at[s - 1], at_x(s)).start()
    lax.fori_loop(0, 8, g_start, 0)
    weight_grads()

    for s in range(NX - 1):
        done(prx.at[s], p_r.at[s])
    total = pr[...] + prx[0] + prx[1] + prx[2]
    for j in range(PLANE):
        prs[j] = total[:, j]
    prr[0] = total[:, 0]
    for j in range(1, PLANE):
        remote(prs.at[j], prr.at[j], pp_s, pp_r, at_plane(j, -1)).start()
    for s in range(NX - 1):
        done(wq.at[s], w_r.at[s])
    done(prr.at[pl.ds(1, PLANE - 1)], pp_r)

    lo_rows, hi_rows = pl.ds(0, 96), pl.ds(96, 96)

    def g_pass(ch):
        done(gx.at[1, ch], g_r.at[0, ch])
        remote(
            gx.at[1, ch, lo_rows], gx.at[3, ch, lo_rows], gf_s.at[0, ch], gf_r.at[0, ch], at_x(1)
        ).start()
        done(gx.at[2, ch], g_r.at[1, ch])
        remote(
            gx.at[2, ch, hi_rows], gx.at[3, ch, hi_rows], gf_s.at[1, ch], gf_r.at[1, ch], at_x(NX - 1)
        ).start()

    def input_grad(ch):
        done(gx.at[3, ch, lo_rows], gf_r.at[0, ch])
        done(gx.at[3, ch, hi_rows], gf_r.at[1, ch])
        first = first_of(FS)
        total = jnp.zeros((ROWS, Q), F32)
        for slot, w in ((0, None), (1, 0), (2, 2), (3, 1)):
            pair = gx[slot, ch].astype(F32)
            gg, ug = pair[:, 0:FS], pair[:, FS:2 * FS]
            lhs = jnp.concatenate(
                [
                    jnp.where(first, gg, 0.0).astype(BF16),
                    jnp.where(first, 0.0, gg).astype(BF16),
                    jnp.where(first, ug, 0.0).astype(BF16),
                    jnp.where(first, 0.0, ug).astype(BF16),
                ],
                axis=1,
            )
            rhs = wgu[x] if w is None else wq[w]
            total = total + lax.dot_general(
                lhs, rhs, (((1,), (1,)), ((), ())), preferred_element_type=F32
            )
        igs[ch] = total
        igr[ch, 0:SLOT] = total[0:SLOT]
        for j in range(1, PLANE):
            at = pl.ds(j * SLOT, SLOT)
            remote(
                igs.at[ch, at], igr.at[ch, at], ig_s.at[ch], ig_r.at[ch], at_plane(j, -1)
            ).start()

    def combine(ch):
        done(igr.at[ch, pl.ds(SLOT, ROWS - SLOT)], ig_r.at[ch])
        row = lax.broadcasted_iota(I32, (ROWS, TOK), 0)
        slots = sl[ch, 0:2]
        p0 = row == slots[0:1]
        p1 = row == slots[1:2]
        pick = (p0 | p1).astype(F32).astype(BF16)
        v = igr[ch]
        hi = v.astype(BF16)
        rest = v - hi.astype(F32)
        mid = rest.astype(BF16)
        low = (rest - mid.astype(F32)).astype(BF16)
        dims = (((0,), (0,)), ((), ()))
        dense = lax.dot_general(pick, hi, dims, preferred_element_type=F32)
        dense = dense + (
            lax.dot_general(pick, mid, dims, preferred_element_type=F32)
            + lax.dot_general(pick, low, dims, preferred_element_type=F32)
        )
        db[ch, 0:TOK] = dense
        spread = jnp.broadcast_to(prr[:, ch][:, None, :], (PLANE, SLOT, FS))
        col = jnp.sum(
            jnp.where(lane_of_slot(), spread, 0.0).reshape(ROWS, FS), axis=1, keepdims=True
        )
        r0 = jnp.sum(jnp.where(p0, col, 0.0), axis=0, keepdims=True)
        r1 = jnp.sum(jnp.where(p1, col, 0.0), axis=0, keepdims=True)
        db[ch, TOK:DENSE] = jnp.concatenate([r0, r1, jnp.zeros((6, Q), F32)], axis=0)

        top, bottom = pl.ds(0, HALF), pl.ds(HALF, DENSE - HALF)

        @pl.when(ch == 4)
        def _():
            remote(db.at[4, top], rm.at[3, top], c_s.at[8], c_r.at[3], at_z(NZ - 1)).start()
            remote(db.at[4, bottom], rp.at[0, bottom], c_s.at[4], c_r.at[4], at_z(1)).start()

        @pl.when(ch == 3)
        def _():
            done(rm.at[3, top], c_r.at[3])
            db[3, top] += rm[3, top]

        @pl.when(ch == 5)
        def _():
            done(rp.at[0, bottom], c_r.at[4])
            db[5, bottom] += rp[0, bottom]

        @pl.when((ch >= 1) & (ch <= 2))
        def _():
            done(rm.at[ch], c_r.at[ch])
            db[ch] += rm[ch]

        @pl.when(ch >= 6)
        def _():
            done(rp.at[ch - 5], c_r.at[ch - 1])
            db[ch] += rp[ch - 5]

        @pl.when((ch >= 1) & (ch <= 3))
        def _():
            remote(db.at[ch], rm.at[ch - 1], c_s.at[ch], c_r.at[ch - 1], at_z(NZ - 1)).start()

        @pl.when(ch >= 5)
        def _():
            remote(db.at[ch], rp.at[ch - 4], c_s.at[ch], c_r.at[ch], at_z(1)).start()

    def back(t, carry):
        @pl.when(t < 8)
        def _():
            g_pass(order(t))

        @pl.when((t >= 1) & (t < 9))
        def _():
            input_grad(order(t - 1))

        @pl.when(t >= 2)
        def _():
            combine(order(t - 2))

        return carry

    lax.fori_loop(0, 10, back, 0)

    done(rm.at[0], c_r.at[0])
    done(rp.at[3], c_r.at[7])
    full = db[0] + (rm[0] + rp[3])
    gg_out[...] = full[TOK:TOK + 2] / gw[...]
    tq[0] = full[0:TOK].astype(BF16)
    remote(tq.at[0], tq.at[1], t_s.at[0], t_r.at[0], at_x(1)).start()
    remote(tq.at[0], tq.at[2], t_s.at[1], t_r.at[1], at_x(NX - 1)).start()
    t_lo, t_hi = pl.ds(0, 128), pl.ds(128, 128)

    def place(slot, who):
        tg_out[:, pl.ds(pl.multiple_of(who * Q, Q), Q)] = tq[slot]

    place(0, x)
    done(tq.at[1], t_r.at[0])
    remote(tq.at[1, t_lo], tq.at[3, t_lo], t_s.at[2], t_r.at[2], at_x(1)).start()
    done(tq.at[2], t_r.at[1])
    remote(tq.at[2, t_hi], tq.at[3, t_hi], t_s.at[3], t_r.at[3], at_x(NX - 1)).start()
    place(1, (x + NX - 1) % NX)
    place(2, (x + 1) % NX)

    for dz in range(NZ):
        for h in range(2):
            if dz <= 3 - h:
                done(bk.at[dz, h], z_s.at[h, dz])
            if dz == 0 or dz >= 6 - h:
                done(bk.at[dz, h], z_s.at[2 + h, dz])
        if dz <= 3:
            done(rb.at[dz], rb_s.at[0, dz])
        if dz == 0 or dz >= 6:
            done(rb.at[dz], rb_s.at[1, dz])
        done(sx.at[dz, :, pl.ds(1, PLANE - 1)], ip_s.at[dz])
        for h in range(2):
            done(rx.at[dz, h], x_s.at[h, dz])
            done(gx.at[0, dz], g_s.at[h, dz])
        done(gx.at[1, dz, lo_rows], gf_s.at[0, dz])
        done(gx.at[2, dz, hi_rows], gf_s.at[1, dz])
        done(igs.at[dz, pl.ds(SLOT, ROWS - SLOT)], ig_s.at[dz])
        if dz in (1, 2, 3, 5, 6, 7):
            done(db.at[dz], c_s.at[dz])
    done(db.at[4, pl.ds(0, HALF)], c_s.at[8])
    done(db.at[4, pl.ds(HALF, DENSE - HALF)], c_s.at[4])
    for s in range(NX - 1):
        done(wq.at[s], w_s.at[s])
        done(pr, p_s.at[s])
    done(prs.at[pl.ds(1, PLANE - 1)], pp_s)
    done(tq.at[0], t_s.at[0])
    done(tq.at[0], t_s.at[1])
    done(tq.at[1, t_lo], t_s.at[2])
    done(tq.at[2, t_hi], t_s.at[3])
    done(tq.at[3, t_lo], t_r.at[2])
    done(tq.at[3, t_hi], t_r.at[3])
    place(3, (x + 2) % NX)


def shards(tokens, cotangent, routing, gate_weights, gate_proj, up_proj, down_proj):
    vmem = pl.BlockSpec(memory_space=pltpu.VMEM)
    dma = pltpu.SemaphoreType.DMA
    scratch = [
        pltpu.VMEM((NZ, 2, 2, TOK, Q), BF16),
        pltpu.VMEM((NZ, 8, TOK), F32),
        pltpu.VMEM((NZ, 2, PLANE, 6, 8, Q), BF16),
        pltpu.VMEM((NZ, 2, PLANE, 6, 8, Q), BF16),
        pltpu.VMEM((NZ, PLANE, 6, 8, Q), BF16),
        pltpu.VMEM((NZ, PLANE, 6, 8, Q), BF16),
        pltpu.VMEM((4, Q, 512), BF16),
        pltpu.VMEM((4, 256, Q), BF16),
        pltpu.VMEM((3, Q, 512), BF16),
        pltpu.VMEM((NZ, 8, TOK), I32),
        pltpu.VMEM((TOK, TOK), BF16),
        pltpu.VMEM((4, 2, ROWS, Q), BF16),
        pltpu.VMEM((ROWS, 512), BF16),
        pltpu.VMEM((ROWS, 256), BF16),
        pltpu.VMEM((4, NZ, ROWS, 256), BF16),
        pltpu.VMEM((NZ, PLANE, FS), F32),
        pltpu.VMEM((3, NZ, PLANE, FS), F32),
        pltpu.VMEM((PLANE, NZ, FS), F32),
        pltpu.VMEM((PLANE, NZ, FS), F32),
        pltpu.VMEM((NZ, ROWS, Q), F32),
        pltpu.VMEM((NZ, ROWS, Q), F32),
        pltpu.VMEM((NZ, DENSE, Q), F32),
        pltpu.VMEM((4, DENSE, Q), F32),
        pltpu.VMEM((4, DENSE, Q), F32),
        pltpu.VMEM((4, TOK, Q), BF16),
        dma((4, 8)), dma((2, 8)), dma((2, 8)), dma((8,)),
        dma((8,)), dma((8,)), dma((2, 8)), dma((2, 8)),
        dma((3,)), dma((3,)), dma((2, 8)), dma((2, 8)), dma((2, 8)), dma((2, 8)),
        dma((3,)), dma((3,)), dma, dma, dma((8,)), dma((8,)),
        dma((9,)), dma((8,)), dma((4,)), dma((4,)),
    ]
    tg, gg, dg, du, dd = pl.pallas_call(
        kernel,
        out_shape=(
            jax.ShapeDtypeStruct((TOK, D), BF16),
            jax.ShapeDtypeStruct((2, TOK), F32),
            jax.ShapeDtypeStruct((2, D, FS), F32),
            jax.ShapeDtypeStruct((2, D, FS), F32),
            jax.ShapeDtypeStruct((2, FS, D), F32),
        ),
        in_specs=[vmem] * 7,
        out_specs=(vmem,) * 5,
        scratch_shapes=scratch,
        compiler_params=pltpu.CompilerParams(
            collective_id=0, has_side_effects=True, vmem_limit_bytes=60 * 1024 * 1024
        ),
    )(tokens, cotangent, routing.T, gate_weights.T, gate_proj, up_proj, down_proj)
    return tg, gg.T, dg, du, dd


def solution(mesh):
    in_specs = (
        P("ep", None),
        P("ep", None),
        P("ep", None),
        P("ep", None),
        P("ep", None, "tp"),
        P("ep", None, "tp"),
        P("ep", "tp", None),
    )
    out_specs = (
        P("ep", None),
        P("ep", None),
        P("ep", None, "tp"),
        P("ep", None, "tp"),
        P("ep", "tp", None),
    )
    return jax.shard_map(shards, mesh=mesh, in_specs=in_specs, out_specs=out_specs, check_vma=False)
```

```python
import jax
import jax.numpy as jnp
from jax import lax
from jax.experimental import pallas as pl
from jax.experimental.pallas import tpu as pltpu
from jax.sharding import PartitionSpec as P

F32 = jnp.float32
BF16 = jnp.bfloat16
I32 = jnp.int32
MESH = pl.DeviceIdType.MESH

NZ, NY, NC, NX = 8, 4, 2, 4
PLANE = NY * NC
TOK = 256
D = 1024
Q = 256
FS = 128
CAP = 12
SLOT = 2 * CAP
ROWS = PLANE * SLOT
ALL = NZ * ROWS
DENSE = TOK + 8
POS = {0: 0, 1: 1, 7: 2, 2: 3, 6: 4, 3: 5, 5: 6, 4: 7}
PARTS = ((0, 128), (128, DENSE - 128))
CONTRACT_MINOR = (((1,), (1,)), ((), ()))
CONTRACT_MAJOR = (((0,), (0,)), ((), ()))


def kernel(
    tok, cot, rt, gw, wg, wu, wd,
    tg_out, gg_out, dg_out, du_out, dd_out,
    bk, rb, other, sx, so, rx, xl, xr, wv, wgu, wds, wq, sl, upper, pk, wt, ts, gu2, h2,
    gx, pr, prx, prs, prr, igs, igr, db, rm, rp, tq, dg, du, dd,
    in_s, z_s, z_r, rb_s, rb_r, ip_s, ip_r, io_s, io_r, x_s, x_r, w_s, w_r, g_s, g_r, gf_s, gf_r,
    p_s, p_r, pp_s, pp_r, ig_s, ig_r, c_s, c_r, t_s, t_r, out_s,
):
    e = lax.axis_index("ep")
    x = lax.axis_index("tp")
    z = e // PLANE
    y = (e % PLANE) // NC
    c = e % NC
    half = x % 2

    def at_z(step):
        return (((z + step) % NZ) * PLANE + y * NC + c, x)

    def at_plane(j, sign):
        dy, dc = j // NC, j % NC
        return (z * PLANE + ((y + sign * dy + NY) % NY) * NC + (c + dc) % NC, x)

    def at_x(step):
        return (e, (x + step) % NX)

    def remote(src, dst, ssem, rsem, dev):
        return pltpu.make_async_remote_copy(
            src_ref=src, dst_ref=dst, send_sem=ssem, recv_sem=rsem,
            device_id=dev, device_id_type=MESH,
        )

    def done(ref, sem):
        pltpu.make_async_copy(ref, ref, sem).wait()

    sends = []

    def push(src, dst, ssem, rsem, dev, last=True):
        remote(src, dst, ssem, rsem, dev).start()
        if last:
            sends.append((src, ssem))

    def quarter(k):
        return 2 * half + k if k < 2 else 2 * (1 - half) + (k - 2)

    with jax.named_scope("prologue"):
        barrier = pltpu.get_barrier_semaphore()
        partners = [at_z(1), at_z(NZ - 1)]
        partners += [at_plane(j, 1) for j in range(1, PLANE)]
        partners += [at_x(s) for s in range(1, NX)]
        for dev in partners:
            pl.semaphore_signal(barrier, inc=1, device_id=dev, device_id_type=MESH)

        loads = []
        for k in range(4):
            cols = pl.ds(pl.multiple_of(quarter(k) * Q, Q), Q)
            dst = bk.at[0, k] if k < 2 else other.at[k - 2]
            loads.append(pltpu.make_async_copy(tok.at[:, cols], dst.at[0], in_s.at[2 * k]))
            loads.append(pltpu.make_async_copy(cot.at[:, cols], dst.at[1], in_s.at[2 * k + 1]))
        for i, w in enumerate((wg, wu)):
            loads.append(pltpu.make_async_copy(w, wv.at[i], in_s.at[8 + i]))
        for q in range(4):
            for i in range(2):
                loads.append(
                    pltpu.make_async_copy(
                        wd.at[i, :, pl.ds(q * Q, Q)], wds.at[q, pl.ds(i * FS, FS)], in_s.at[10 + 2 * q + i]
                    )
                )
        for load in loads:
            load.start()
        rb[0] = jnp.concatenate(
            [rt[...].astype(F32), gw[...], jnp.zeros((4, TOK), F32)], axis=0
        )
        upper[...] = (
            lax.broadcasted_iota(I32, (TOK, TOK), 0) < lax.broadcasted_iota(I32, (TOK, TOK), 1)
        ).astype(F32).astype(BF16)
        for load in loads[:4]:
            load.wait()
    with jax.named_scope("barrier"):
        pl.semaphore_wait(barrier, len(partners))

    def first_of(n, lanes):
        i = lax.broadcasted_iota(I32, (n * PLANE, SLOT, lanes), 1)
        return (i < CAP).reshape(n * ROWS, lanes)

    def lane_of_slot(n):
        i = lax.broadcasted_iota(I32, (n * PLANE, SLOT, FS), 1)
        l = lax.broadcasted_iota(I32, (n * PLANE, SLOT, FS), 2)
        return i == l

    def z_push(dz, h, plus):
        if plus:
            to, dev, i = dz + 1, at_z(1), h
        else:
            to, dev, i = (dz + NZ - 1) % NZ, at_z(NZ - 1), 2 + h
        push(bk.at[dz, h], bk.at[to, h], z_s.at[i, dz], z_r.at[h, to], dev)

    def rb_push(dz, plus):
        if plus:
            to, dev, i = dz + 1, at_z(1), 0
        else:
            to, dev, i = (dz + NZ - 1) % NZ, at_z(NZ - 1), 1
        push(rb.at[dz], rb.at[to], rb_s.at[i, dz], rb_r.at[to], dev)

    @jax.named_scope("slots_of")
    def slots_of(dz):
        pos = POS[dz]
        e16 = lax.broadcasted_iota(I32, (16, TOK), 0)
        target = ((e16 // 4 - y) & 3) * NC + (((e16 // 2) - c) & 1)
        base = (target * SLOT + (e16 & 1) * CAP).astype(F32)
        block = rb[dz]
        chosen = block[0:2].astype(I32) - z * 16
        e0 = (e16 == chosen[0:1]).astype(F32)
        e1 = (e16 == chosen[1:2]).astype(F32)
        both = jnp.concatenate([e0, e1], axis=0).astype(BF16)
        before = jnp.dot(both, upper[...], preferred_element_type=F32)
        before0 = before[0:16]
        before1 = before[16:32] + jnp.sum(e0, axis=1, keepdims=True)
        s0 = jnp.sum(e0 * (base + before0 + 1.0), axis=0, keepdims=True) - 1.0
        s1 = jnp.sum(e1 * (base + before1 + 1.0), axis=0, keepdims=True) - 1.0
        slots = jnp.concatenate([s0, s1], axis=0).astype(I32)
        sl[pos, 0:2] = slots
        row = lax.broadcasted_iota(I32, (ROWS, TOK), 0)
        p0 = row == slots[0:1]
        p1 = row == slots[1:2]
        pk[pos] = (p0 | p1).astype(F32).astype(BF16)
        weight = jnp.sum(
            jnp.where(p0, block[2:3], 0.0) + jnp.where(p1, block[3:4], 0.0),
            axis=1, keepdims=True,
        )
        wt[pos] = jnp.broadcast_to(weight, (ROWS, FS))

    @jax.named_scope("build")
    def build(dz, h, src, stage, land, ssem, rsem):
        pos = POS[dz]
        pick = pk[pos]
        w = jnp.concatenate([wt[pos], wt[pos]], axis=1)
        t = jnp.dot(pick, src[0], preferred_element_type=F32)
        s = jnp.dot(pick, src[1], preferred_element_type=F32) * w
        t = t.reshape(PLANE, 3, 8, Q).astype(BF16)
        s = s.reshape(PLANE, 3, 8, Q).astype(BF16)
        stage[:, 0:3] = t
        stage[:, 3:6] = s
        land[0, 0:3] = t[0]
        land[0, 3:6] = s[0]
        for j in range(1, PLANE):
            push(stage.at[j], land.at[j], ssem, rsem, at_plane(j, 1), last=False)
        sends.append((stage.at[pl.ds(1, PLANE - 1)], ssem))

    def build_half(dz, h):
        pos = POS[dz]
        build(dz, h, bk.at[dz, h], sx.at[pos, h], rx.at[h, pos], ip_s.at[h, pos], ip_r.at[h, pos])

    @jax.named_scope("x_push")
    def x_push(dz, h):
        pos = POS[dz]
        done(rx.at[h, pos, pl.ds(1, PLANE - 1)], ip_r.at[h, pos])
        dst = xl if h == 0 else xr
        push(rx.at[h, pos], dst.at[pos], x_s.at[h, pos], x_r.at[h, pos], at_x(1 if h == 0 else NX - 1))

    @jax.named_scope("compute_wait")
    def compute_wait(p, n):
        for i in range(p, p + n):
            if i == 0:
                for h in range(2):
                    done(rx.at[h, 0, pl.ds(1, PLANE - 1)], ip_r.at[h, 0])
                done(xl.at[0, pl.ds(1, PLANE - 1)], io_r.at[0])
                done(xr.at[0, pl.ds(1, PLANE - 1)], io_r.at[1])
            else:
                done(xl.at[i], x_r.at[0, i])
                done(xr.at[i], x_r.at[1, i])

    @jax.named_scope("compute")
    def compute(p, n):
        m = n * ROWS
        rows = pl.ds(p * ROWS, m)
        pre = jnp.zeros((m, 512), F32)
        hg = jnp.zeros((m, 256), F32)
        for k, src in enumerate((rx.at[0], rx.at[1], xl, xr)):
            t = src[p:p + n, :, 0:3].astype(F32).reshape(m, Q).astype(BF16)
            s = src[p:p + n, :, 3:6].astype(F32).reshape(m, Q).astype(BF16)
            ts[k, 0, rows] = t
            ts[k, 1, rows] = s
            pre = pre + jnp.dot(t, wgu[quarter(k)], preferred_element_type=F32)
            hg = hg + lax.dot_general(
                s, wds[quarter(k)], CONTRACT_MINOR, preferred_element_type=F32
            )
        first = first_of(n, FS)
        g = jnp.where(first, pre[:, 0:128], pre[:, 128:256]).astype(BF16).astype(F32)
        u = jnp.where(first, pre[:, 256:384], pre[:, 384:512]).astype(BF16).astype(F32)
        dh = jnp.where(first, hg[:, 0:128], hg[:, 128:256])
        sg = jax.nn.sigmoid(g)
        act = g * sg
        hidden = act * u
        product = jnp.sum(dh * hidden, axis=1, keepdims=True)
        placed = jnp.where(
            lane_of_slot(n),
            jnp.broadcast_to(product, (m, FS)).reshape(n * PLANE, SLOT, FS),
            0.0,
        )
        pr[p:p + n] = jnp.sum(placed, axis=1).reshape(n, PLANE, FS)
        gg = dh * u * sg * (1.0 + g * (1.0 - sg))
        ug = dh * act
        gx[0, rows, 0:FS] = gg.astype(BF16)
        gx[0, rows, FS:2 * FS] = ug.astype(BF16)
        for i, v in enumerate((gg, ug, hidden)):
            lo = jnp.where(first, v, 0.0).astype(BF16)
            hi = jnp.where(first, 0.0, v).astype(BF16)
            if i < 2:
                gu2[rows, 256 * i:256 * i + 128] = lo
                gu2[rows, 256 * i + 128:256 * i + 256] = hi
            else:
                h2[rows, 0:128] = lo
                h2[rows, 128:256] = hi

    @jax.named_scope("weight_grads")
    def weight_grads(k):
        at = pl.ds(pl.multiple_of(quarter(k) * Q, Q), Q)
        o = lax.dot_general(ts[k, 0], gu2[...], CONTRACT_MAJOR, preferred_element_type=F32)
        for i in range(2):
            dg[i, at, :] = o[:, i * FS:(i + 1) * FS]
            du[i, at, :] = o[:, 256 + i * FS:256 + (i + 1) * FS]
        o = lax.dot_general(h2[...], ts[k, 1], CONTRACT_MAJOR, preferred_element_type=F32)
        for i in range(2):
            dd[i, :, at] = o[i * FS:(i + 1) * FS]

    def rows_of(dz, lo=0, n=ROWS):
        return pl.ds(POS[dz] * ROWS + lo, n)

    def g_push(dz):
        r = rows_of(dz)
        push(gx.at[0, r], gx.at[1, r], g_s.at[0, dz], g_r.at[0, dz], at_x(1))
        push(gx.at[0, r], gx.at[2, r], g_s.at[1, dz], g_r.at[1, dz], at_x(NX - 1))

    @jax.named_scope("g_pass")
    def g_pass(dz):
        lo, hi = rows_of(dz, 0, 96), rows_of(dz, 96, 96)
        done(gx.at[1, rows_of(dz)], g_r.at[0, dz])
        push(gx.at[1, lo], gx.at[3, lo], gf_s.at[0, dz], gf_r.at[0, dz], at_x(1))
        done(gx.at[2, rows_of(dz)], g_r.at[1, dz])
        push(gx.at[2, hi], gx.at[3, hi], gf_s.at[1, dz], gf_r.at[1, dz], at_x(NX - 1))

    @jax.named_scope("ig_wait")
    def ig_wait(dz):
        done(gx.at[3, rows_of(dz, 0, 96)], gf_r.at[0, dz])
        done(gx.at[3, rows_of(dz, 96, 96)], gf_r.at[1, dz])

    @jax.named_scope("input_grad")
    def input_grad(dz):
        pos = POS[dz]
        first = first_of(1, FS)
        total = jnp.zeros((ROWS, Q), F32)
        for slot, w in ((0, None), (1, 0), (2, 2), (3, 1)):
            pair = gx[slot, rows_of(dz)].astype(F32)
            gg, ug = pair[:, 0:FS], pair[:, FS:2 * FS]
            lhs = jnp.concatenate(
                [
                    jnp.where(first, gg, 0.0).astype(BF16),
                    jnp.where(first, 0.0, gg).astype(BF16),
                    jnp.where(first, ug, 0.0).astype(BF16),
                    jnp.where(first, 0.0, ug).astype(BF16),
                ],
                axis=1,
            )
            rhs = wgu[x] if w is None else wq[w]
            total = total + lax.dot_general(lhs, rhs, CONTRACT_MINOR, preferred_element_type=F32)
        igs[pos] = total
        igr[pos, 0:SLOT] = total[0:SLOT]
        for j in range(1, PLANE):
            at = pl.ds(j * SLOT, SLOT)
            push(
                igs.at[pos, at], igr.at[pos, at], ig_s.at[pos], ig_r.at[pos], at_plane(j, -1),
                last=False,
            )
        sends.append((igs.at[pos, pl.ds(SLOT, ROWS - SLOT)], ig_s.at[pos]))

    @jax.named_scope("dense")
    def dense(dz):
        pos = POS[dz]
        with jax.named_scope("dense_wait"):
            done(igr.at[pos, pl.ds(SLOT, ROWS - SLOT)], ig_r.at[pos])
        pick = pk[pos]
        v = igr[pos]
        hi = v.astype(BF16)
        rest = v - hi.astype(F32)
        mid = rest.astype(BF16)
        low = (rest - mid.astype(F32)).astype(BF16)
        total = lax.dot_general(pick, hi, CONTRACT_MAJOR, preferred_element_type=F32)
        total = total + (
            lax.dot_general(pick, mid, CONTRACT_MAJOR, preferred_element_type=F32)
            + lax.dot_general(pick, low, CONTRACT_MAJOR, preferred_element_type=F32)
        )
        db[dz, 0:TOK] = total
        row = lax.broadcasted_iota(I32, (ROWS, TOK), 0)
        slots = sl[pos, 0:2]
        spread = jnp.broadcast_to(prr[:, pos][:, None, :], (PLANE, SLOT, FS))
        col = jnp.sum(
            jnp.where(lane_of_slot(1), spread, 0.0).reshape(ROWS, FS), axis=1, keepdims=True
        )
        r0 = jnp.sum(jnp.where(row == slots[0:1], col, 0.0), axis=0, keepdims=True)
        r1 = jnp.sum(jnp.where(row == slots[1:2], col, 0.0), axis=0, keepdims=True)
        db[dz, TOK:DENSE] = jnp.concatenate([r0, r1, jnp.zeros((6, Q), F32)], axis=0)

    def part(i):
        return pl.ds(*PARTS[i])

    @jax.named_scope("chain")
    def chain(dz):
        if dz == 4:
            push(db.at[4, part(0)], rm.at[3, part(0)], c_s.at[0, 4], c_r.at[0, 3], at_z(NZ - 1))
            push(db.at[4, part(1)], rp.at[0, part(1)], c_s.at[1, 4], c_r.at[1, 4], at_z(1))
        elif dz < 4:
            for i in (1, 0):
                if dz < 3 or i == 0:
                    done(rm.at[dz, part(i)], c_r.at[i, dz])
                    db[dz, part(i)] += rm[dz, part(i)]
                push(
                    db.at[dz, part(i)], rm.at[dz - 1, part(i)], c_s.at[i, dz], c_r.at[i, dz - 1],
                    at_z(NZ - 1),
                )
        else:
            for i in (0, 1):
                if dz > 5 or i == 1:
                    done(rp.at[dz - 5, part(i)], c_r.at[i, dz - 1])
                    db[dz, part(i)] += rp[dz - 5, part(i)]
                push(
                    db.at[dz, part(i)], rp.at[dz - 4, part(i)], c_s.at[i, dz], c_r.at[i, dz],
                    at_z(1),
                )

    for h in range(2):
        z_push(0, h, True)
        z_push(0, 1 - h, False)
        if h == 0:
            rb_push(0, True)
            rb_push(0, False)
    slots_of(0)
    for h in range(2):
        build_half(0, h)
    for load in loads[4:10]:
        load.wait()
    for h in range(2):
        build(
            0, h, other.at[h], so.at[h], (xl if h == 0 else xr).at[0], io_s.at[h], io_r.at[h]
        )
    with jax.named_scope("weights"):
        for q in range(4):
            for w in range(2):
                for i in range(2):
                    lane = 256 * w + FS * i
                    wgu[q, :, lane:lane + FS] = wv[w, i, q * Q:(q + 1) * Q, :]
        for s in range(1, NX):
            push(wgu.at[(x + s) % NX], wq.at[s - 1], w_s.at[s - 1], w_r.at[s - 1], at_x(s))
        for load in loads[10:]:
            load.wait()

    def arrivals(s):
        k = (s + 1) // 2
        if s == 7:
            return ((4, 0), (4, 1))
        return ((k, 0), (NZ - k, 1)) if s % 2 else ((k, 1), (NZ - k, 0))

    for s in range(1, 8):
        here = arrivals(s)
        with jax.named_scope("z_wait"):
            for i, (dz, h) in enumerate(here):
                if s % 2 and not (s == 7 and i == 1):
                    done(rb.at[dz], rb_r.at[dz])
                    if s == 7:
                        pass
                    elif i == 0:
                        rb_push(dz, True)
                    elif s < 5:
                        rb_push(dz, False)
                done(bk.at[dz, h], z_r.at[h, dz])
                if s < 6:
                    z_push(dz, h, i == 0)
        if s % 2:
            for dz in dict.fromkeys(dz for dz, _ in here):
                slots_of(dz)
        for dz, h in here:
            build_half(dz, h)
        if s > 1:
            for dz, h in arrivals(s - 1):
                x_push(dz, h)
        if s == 2:
            compute_wait(0, 1)
            compute(0, 1)
            g_push(0)
        if s == 4:
            g_pass(0)
            compute_wait(1, 2)
            compute(1, 2)
        if s == 6:
            compute_wait(3, 2)
            compute(3, 2)
        if s == 5:
            with jax.named_scope("wq_wait"):
                for i in range(NX - 1):
                    done(wq.at[i], w_r.at[i])
            ig_wait(0)
            input_grad(0)
    for dz, h in arrivals(7):
        x_push(dz, h)
    compute_wait(5, 2)
    compute(5, 2)
    compute_wait(7, 1)
    compute(7, 1)

    back = (4, 3, 5, 2, 6, 1, 7)
    for dz in back[:3]:
        g_push(dz)
    for s in range(1, NX):
        push(pr, prx.at[s - 1], p_s.at[s - 1], p_r.at[s - 1], at_x(s))
    weight_grads(0)

    def products():
        with jax.named_scope("products"):
            for s in range(NX - 1):
                done(prx.at[s], p_r.at[s])
            total = pr[...] + prx[0] + prx[1] + prx[2]
            for j in range(PLANE):
                prs[j] = total[:, j]
            prr[0] = total[:, 0]
            for j in range(1, PLANE):
                push(prs.at[j], prr.at[j], pp_s, pp_r, at_plane(j, -1), last=False)
            sends.append((prs.at[pl.ds(1, PLANE - 1)], pp_s))

    outs = []

    def put(src, dst, sem):
        copy = pltpu.make_async_copy(src, dst, sem)
        copy.start()
        outs.append(copy)

    chains = {2: (4,), 4: (3, 5), 6: (2,), 7: (6,)}
    for i in range(8):
        if i < 7:
            g_pass(back[i])
            if i + 3 < 7:
                g_push(back[i + 3])
        if i == 0:
            products()
        if 1 <= i <= 7:
            ig_wait(back[i - 1])
            input_grad(back[i - 1])
        if i in (1, 2, 3):
            weight_grads(i)
        if i == 1:
            with jax.named_scope("products_wait"):
                done(prr.at[pl.ds(1, PLANE - 1)], pp_r)
        if i == 3:
            put(dg, dg_out, out_s.at[0])
            put(du, du_out, out_s.at[1])
            put(dd, dd_out, out_s.at[2])
        if i >= 2:
            dense(back[i - 2])
        if i == 3:
            dense(0)
        for dz in chains.get(i, ()):
            chain(dz)
    dense(7)
    chain(1)
    chain(7)

    t_rows = (pl.ds(0, 128), pl.ds(128, 128))
    with jax.named_scope("final"):
        for i in (0, 1):
            done(rm.at[0, part(i)], c_r.at[i, 0])
            done(rp.at[3, part(i)], c_r.at[i, 7])
            full = db[0, part(i)] + (rm[0, part(i)] + rp[3, part(i)])
            tq[0, t_rows[i]] = full[0:128].astype(BF16)
            push(tq.at[0, t_rows[i]], tq.at[1, t_rows[i]], t_s.at[0, i], t_r.at[0, i], at_x(1))
            push(tq.at[0, t_rows[i]], tq.at[2, t_rows[i]], t_s.at[1, i], t_r.at[1, i], at_x(NX - 1))
            if i == 1:
                gg_out[...] = full[128:130] / gw[...]

    def place(slot, who, sem):
        put(tq.at[slot], tg_out.at[:, pl.ds(pl.multiple_of(who * Q, Q), Q)], sem)

    with jax.named_scope("gather"):
        place(0, x, out_s.at[3])
        done(tq.at[1, t_rows[0]], t_r.at[0, 0])
        push(tq.at[1, t_rows[0]], tq.at[3, t_rows[0]], t_s.at[2, 0], t_r.at[2, 0], at_x(1))
        done(tq.at[2, t_rows[0]], t_r.at[1, 0])
        done(tq.at[2, t_rows[1]], t_r.at[1, 1])
        push(tq.at[2, t_rows[1]], tq.at[3, t_rows[1]], t_s.at[2, 1], t_r.at[2, 1], at_x(NX - 1))
        done(tq.at[1, t_rows[1]], t_r.at[0, 1])
        place(1, (x + NX - 1) % NX, out_s.at[4])
        place(2, (x + 1) % NX, out_s.at[5])
    with jax.named_scope("drain"):
        for src, sem in sends:
            done(src, sem)
        for i in range(2):
            done(tq.at[3, t_rows[i]], t_r.at[2, i])
        place(3, (x + 2) % NX, out_s.at[6])
        for copy in outs:
            copy.wait()


def shards(tokens, cotangent, routing, gate_weights, gate_proj, up_proj, down_proj):
    vmem = pl.BlockSpec(memory_space=pltpu.VMEM)
    hbm = pl.BlockSpec(memory_space=pl.ANY)
    dma = pltpu.SemaphoreType.DMA
    scratch = [
        pltpu.VMEM((NZ, 2, 2, TOK, Q), BF16),
        pltpu.VMEM((NZ, 8, TOK), F32),
        pltpu.VMEM((2, 2, TOK, Q), BF16),
        pltpu.VMEM((NZ, 2, PLANE, 6, 8, Q), BF16),
        pltpu.VMEM((2, PLANE, 6, 8, Q), BF16),
        pltpu.VMEM((2, NZ, PLANE, 6, 8, Q), BF16),
        pltpu.VMEM((NZ, PLANE, 6, 8, Q), BF16),
        pltpu.VMEM((NZ, PLANE, 6, 8, Q), BF16),
        pltpu.VMEM((2, 2, D, FS), BF16),
        pltpu.VMEM((4, Q, 512), BF16),
        pltpu.VMEM((4, 256, Q), BF16),
        pltpu.VMEM((3, Q, 512), BF16),
        pltpu.VMEM((NZ, 8, TOK), I32),
        pltpu.VMEM((TOK, TOK), BF16),
        pltpu.VMEM((NZ, ROWS, TOK), BF16),
        pltpu.VMEM((NZ, ROWS, FS), F32),
        pltpu.VMEM((4, 2, ALL, Q), BF16),
        pltpu.VMEM((ALL, 512), BF16),
        pltpu.VMEM((ALL, 256), BF16),
        pltpu.VMEM((4, ALL, 256), BF16),
        pltpu.VMEM((NZ, PLANE, FS), F32),
        pltpu.VMEM((3, NZ, PLANE, FS), F32),
        pltpu.VMEM((PLANE, NZ, FS), F32),
        pltpu.VMEM((PLANE, NZ, FS), F32),
        pltpu.VMEM((NZ, ROWS, Q), F32),
        pltpu.VMEM((NZ, ROWS, Q), F32),
        pltpu.VMEM((NZ, DENSE, Q), F32),
        pltpu.VMEM((4, DENSE, Q), F32),
        pltpu.VMEM((4, DENSE, Q), F32),
        pltpu.VMEM((4, TOK, Q), BF16),
        pltpu.VMEM((2, D, FS), F32),
        pltpu.VMEM((2, D, FS), F32),
        pltpu.VMEM((2, FS, D), F32),
        dma((18,)), dma((4, 8)), dma((2, 8)), dma((2, 8)), dma((8,)),
        dma((2, 8)), dma((2, 8)), dma((2,)), dma((2,)), dma((2, 8)), dma((2, 8)),
        dma((3,)), dma((3,)), dma((2, 8)), dma((2, 8)), dma((2, 8)), dma((2, 8)),
        dma((3,)), dma((3,)), dma, dma, dma((8,)), dma((8,)),
        dma((2, 8)), dma((2, 8)), dma((3, 2)), dma((3, 2)), dma((7,)),
    ]
    tg, gg, dg, du, dd = pl.pallas_call(
        kernel,
        out_shape=(
            jax.ShapeDtypeStruct((TOK, D), BF16),
            jax.ShapeDtypeStruct((2, TOK), F32),
            jax.ShapeDtypeStruct((2, D, FS), F32),
            jax.ShapeDtypeStruct((2, D, FS), F32),
            jax.ShapeDtypeStruct((2, FS, D), F32),
        ),
        in_specs=[hbm, hbm, vmem, vmem, hbm, hbm, hbm],
        out_specs=(hbm, vmem, hbm, hbm, hbm),
        scratch_shapes=scratch,
        compiler_params=pltpu.CompilerParams(
            collective_id=0, has_side_effects=True, vmem_limit_bytes=63 * 1024 * 1024
        ),
    )(tokens, cotangent, routing.T, gate_weights.T, gate_proj, up_proj, down_proj)
    return tg, gg.T, dg, du, dd


def solution(mesh):
    in_specs = (
        P("ep", None),
        P("ep", None),
        P("ep", None),
        P("ep", None),
        P("ep", None, "tp"),
        P("ep", None, "tp"),
        P("ep", "tp", None),
    )
    out_specs = (
        P("ep", None),
        P("ep", None),
        P("ep", None, "tp"),
        P("ep", None, "tp"),
        P("ep", "tp", None),
    )
    return jax.shard_map(shards, mesh=mesh, in_specs=in_specs, out_specs=out_specs, check_vma=False)
```

```python
import jax
import jax.numpy as jnp
from jax import lax
from jax.experimental import pallas as pl
from jax.experimental.pallas import tpu as pltpu
from jax.sharding import PartitionSpec as P

F32 = jnp.float32
BF16 = jnp.bfloat16
I32 = jnp.int32
MESH = pl.DeviceIdType.MESH

NZ, NY, NC, NX = 8, 4, 2, 4
PLANE = NY * NC
TOK = 256
D = 1024
Q = 256
FS = 128
CAP = 12
SLOT = 2 * CAP
ROWS = PLANE * SLOT
ALL = NZ * ROWS
POS = {0: 0, 1: 1, 7: 2, 2: 3, 6: 4, 3: 5, 5: 6, 4: 7}
BRINGS = {
    0: (0, 3), 1: (0, 3, 2), 2: (0, 3), 3: (0, 3), 4: (0,), 5: (0, 3), 6: (0, 3), 7: (0, 3, 1),
}
HELD = [(0, k) for k in range(4)]
HELD += [(dz, k) for dz in range(1, NZ) for k in BRINGS[dz]]
HELD = {key: i for i, key in enumerate(HELD)}
BUILT = {key: i for i, key in enumerate((dz, k) for dz in range(NZ) for k in BRINGS[dz])}
PART = TOK // 4
CONTRACT_MINOR = (((1,), (1,)), ((), ()))
CONTRACT_MAJOR = (((0,), (0,)), ((), ()))


def kernel(
    tok, cot, rt, gw, wg, wu, wd,
    tg_out, gg_out, dg_out, du_out, dd_out,
    bk, rb, sx, rq, wv, wgu, wds, wq, sl, upper, pk, wt, ts, gu2, h2,
    gx, pr, prx, prs, prr, pb, pe, igs, igr, db, rm, rp, tq, dg, du, dd,
    in_s, z_s, z_r, rb_s, rb_r, ip_s, ip_r, x_s, x_r, xf_s, xf_r, w_s, w_r, g_s, g_r, gf_s, gf_r,
    p_s, p_r, pp_s, pp_r, pz_s, pz_r, ig_s, ig_r, c_s, c_r, t_s, t_r, out_s,
):
    e = lax.axis_index("ep")
    x = lax.axis_index("tp")
    z = e // PLANE
    y = (e % PLANE) // NC
    c = e % NC

    def at_z(step):
        return (((z + step) % NZ) * PLANE + y * NC + c, x)

    def at_plane(j, sign):
        dy, dc = j // NC, j % NC
        return (z * PLANE + ((y + sign * dy + NY) % NY) * NC + (c + dc) % NC, x)

    def at_x(step):
        return (e, (x + step) % NX)

    def remote(src, dst, ssem, rsem, dev):
        return pltpu.make_async_remote_copy(
            src_ref=src, dst_ref=dst, send_sem=ssem, recv_sem=rsem,
            device_id=dev, device_id_type=MESH,
        )

    def done(ref, sem):
        pltpu.make_async_copy(ref, ref, sem).wait()

    sends = []

    def push(src, dst, ssem, rsem, dev, last=True):
        remote(src, dst, ssem, rsem, dev).start()
        if last:
            sends.append((src, ssem))

    def quarter(k):
        who = (x + (0, NX - 1, 1, 2)[k]) % NX
        return 2 * (who % 2) + who // 2

    with jax.named_scope("prologue"):
        barrier = pltpu.get_barrier_semaphore()
        partners = [at_z(k) for k in range(1, NZ)]
        partners += [at_plane(j, 1) for j in range(1, PLANE)]
        partners += [at_x(s) for s in range(1, NX)]
        for dev in partners:
            pl.semaphore_signal(barrier, inc=1, device_id=dev, device_id_type=MESH)

        loads = []
        for k in (0, 3, 1, 2):
            cols = pl.ds(pl.multiple_of(quarter(k) * Q, Q), Q)
            dst = bk.at[HELD[0, k]]
            loads.append(pltpu.make_async_copy(tok.at[:, cols], dst.at[0], in_s.at[2 * k]))
            loads.append(pltpu.make_async_copy(cot.at[:, cols], dst.at[1], in_s.at[2 * k + 1]))
        for i, w in enumerate((wg, wu)):
            loads.append(pltpu.make_async_copy(w, wv.at[i], in_s.at[8 + i]))
        for q in range(4):
            for i in range(2):
                loads.append(
                    pltpu.make_async_copy(
                        wd.at[i, :, pl.ds(q * Q, Q)], wds.at[q, pl.ds(i * FS, FS)], in_s.at[10 + 2 * q + i]
                    )
                )
        for load in loads:
            load.start()
        rb[0] = jnp.concatenate(
            [rt[...].astype(F32), gw[...], jnp.zeros((4, TOK), F32)], axis=0
        )
        upper[...] = (
            lax.broadcasted_iota(I32, (TOK, TOK), 0) < lax.broadcasted_iota(I32, (TOK, TOK), 1)
        ).astype(F32).astype(BF16)
        pr[...] = jnp.zeros_like(pr)
        for load in loads[:4]:
            load.wait()
    with jax.named_scope("barrier"):
        pl.semaphore_wait(barrier, len(partners))

    def first_of(n, lanes):
        i = lax.broadcasted_iota(I32, (n * PLANE, SLOT, lanes), 1)
        return (i < CAP).reshape(n * ROWS, lanes)

    def lane_of_slot(pos):
        i = lax.broadcasted_iota(I32, (PLANE, SLOT, FS), 1)
        l = lax.broadcasted_iota(I32, (PLANE, SLOT, FS), 2)
        return i + 32 * (pos % 4) == l

    def toward(dz, plus):
        return (dz + 1, at_z(1)) if plus else ((dz + NZ - 1) % NZ, at_z(NZ - 1))

    def z_push(dz, k, plus):
        to, dev = toward(dz, plus)
        src, i = bk.at[HELD[dz, k]], HELD[to, k]
        if to == 4:
            a = 0 if plus else 1
            push(src.at[a], bk.at[i, a], z_s.at[a, HELD[dz, k]], z_r.at[a, i], dev)
        else:
            push(src, bk.at[i], z_s.at[0 if plus else 1, HELD[dz, k]], z_r.at[0, i], dev)

    @jax.named_scope("z_take")
    def z_take(dz, k, onward=True):
        i = HELD[dz, k]
        plus = dz < 4
        first = k == 0
        if first:
            done(rb.at[dz], rb_r.at[dz])
            if dz < 4 or dz > 5:
                if dz != 4:
                    rb_push(dz, plus)
        if dz == 4:
            for a in range(2):
                done(bk.at[i, a], z_r.at[a, i])
            return
        done(bk.at[i], z_r.at[0, i])
        if k in BRINGS[toward(dz, plus)[0]]:
            z_push(dz, k, plus)

    def rb_push(dz, plus):
        if plus:
            to, dev, i = dz + 1, at_z(1), 0
        else:
            to, dev, i = (dz + NZ - 1) % NZ, at_z(NZ - 1), 1
        push(rb.at[dz], rb.at[to], rb_s.at[i, dz], rb_r.at[to], dev)

    @jax.named_scope("slots_of")
    def slots_of(dz):
        pos = POS[dz]
        e16 = lax.broadcasted_iota(I32, (16, TOK), 0)
        target = ((e16 // 4 - y) & 3) * NC + (((e16 // 2) - c) & 1)
        base = (target * SLOT + (e16 & 1) * CAP).astype(F32)
        block = rb[dz]
        chosen = block[0:2].astype(I32) - z * 16
        e0 = (e16 == chosen[0:1]).astype(F32)
        e1 = (e16 == chosen[1:2]).astype(F32)
        both = jnp.concatenate([e0, e1], axis=0).astype(BF16)
        before = jnp.dot(both, upper[...], preferred_element_type=F32)
        before0 = before[0:16]
        before1 = before[16:32] + jnp.sum(e0, axis=1, keepdims=True)
        s0 = jnp.sum(e0 * (base + before0 + 1.0), axis=0, keepdims=True) - 1.0
        s1 = jnp.sum(e1 * (base + before1 + 1.0), axis=0, keepdims=True) - 1.0
        slots = jnp.concatenate([s0, s1], axis=0).astype(I32)
        sl[pos, 0:2] = slots
        row = lax.broadcasted_iota(I32, (ROWS, TOK), 0)
        p0 = row == slots[0:1]
        p1 = row == slots[1:2]
        pk[pos] = (p0 | p1).astype(F32).astype(BF16)
        weight = jnp.sum(
            jnp.where(p0, block[2:3], 0.0) + jnp.where(p1, block[3:4], 0.0),
            axis=1, keepdims=True,
        )
        wt[pos] = jnp.broadcast_to(weight, (ROWS, FS))

    @jax.named_scope("build")
    def build(dz, k):
        pos, b = POS[dz], BUILT[dz, k]
        src, stage, land = bk.at[HELD[dz, k]], sx.at[b], rq.at[k, pos]
        pick = pk[pos]
        w = jnp.concatenate([wt[pos], wt[pos]], axis=1)
        t = jnp.dot(pick, src[0], preferred_element_type=F32)
        s = jnp.dot(pick, src[1], preferred_element_type=F32) * w
        t = t.reshape(PLANE, 3, 8, Q).astype(BF16)
        s = s.reshape(PLANE, 3, 8, Q).astype(BF16)
        stage[:, 0:3] = t
        stage[:, 3:6] = s
        land[0, 0:3] = t[0]
        land[0, 3:6] = s[0]
        for j in range(1, PLANE):
            push(stage.at[j], land.at[j], ip_s.at[b], ip_r.at[b], at_plane(j, 1), last=False)
        sends.append((stage.at[pl.ds(1, PLANE - 1)], ip_s.at[b]))

    def landed(dz, k):
        done(rq.at[k, POS[dz], pl.ds(1, PLANE - 1)], ip_r.at[BUILT[dz, k]])

    @jax.named_scope("x_push")
    def x_push(dz):
        pos = POS[dz]
        landed(dz, 0)
        if 1 not in BRINGS[dz]:
            push(rq.at[0, pos], rq.at[1, pos], x_s.at[0, pos], x_r.at[0, pos], at_x(1))
        if 2 not in BRINGS[dz]:
            push(rq.at[0, pos], rq.at[2, pos], x_s.at[1, pos], x_r.at[1, pos], at_x(NX - 1))

    low, high = pl.ds(0, PLANE // 2), pl.ds(PLANE // 2, PLANE // 2)

    @jax.named_scope("x_pass")
    def x_pass(dz):
        pos = POS[dz]
        done(rq.at[1, pos], x_r.at[0, pos])
        push(rq.at[1, pos, low], rq.at[3, pos, low], xf_s.at[0, pos], xf_r.at[0, pos], at_x(1))
        done(rq.at[2, pos], x_r.at[1, pos])
        push(
            rq.at[2, pos, high], rq.at[3, pos, high], xf_s.at[1, pos], xf_r.at[1, pos],
            at_x(NX - 1),
        )

    @jax.named_scope("compute_wait")
    def compute_wait(*blocks):
        for dz in blocks:
            pos, own = POS[dz], BRINGS[dz]
            for k in own[1:]:
                landed(dz, k)
            if 3 not in own:
                done(rq.at[3, pos, low], xf_r.at[0, pos])
                done(rq.at[3, pos, high], xf_r.at[1, pos])
            else:
                for k in (1, 2):
                    if k not in own:
                        done(rq.at[k, pos], x_r.at[k - 1, pos])

    @jax.named_scope("compute")
    def compute(*blocks):
        p, n = POS[blocks[0]], len(blocks)
        m = n * ROWS
        rows = pl.ds(p * ROWS, m)
        pre = jnp.zeros((m, 512), F32)
        hg = jnp.zeros((m, 256), F32)
        for k in range(4):
            src = rq.at[k]
            t = src[p:p + n, :, 0:3].astype(F32).reshape(m, Q).astype(BF16)
            s = src[p:p + n, :, 3:6].astype(F32).reshape(m, Q).astype(BF16)
            ts[k, 0, rows] = t
            ts[k, 1, rows] = s
            pre = pre + jnp.dot(t, wgu[quarter(k)], preferred_element_type=F32)
            hg = hg + lax.dot_general(
                s, wds[quarter(k)], CONTRACT_MINOR, preferred_element_type=F32
            )
        first = first_of(n, FS)
        g = jnp.where(first, pre[:, 0:128], pre[:, 128:256]).astype(BF16).astype(F32)
        u = jnp.where(first, pre[:, 256:384], pre[:, 384:512]).astype(BF16).astype(F32)
        dh = jnp.where(first, hg[:, 0:128], hg[:, 128:256])
        sg = jax.nn.sigmoid(g)
        act = g * sg
        hidden = act * u
        product = jnp.sum(dh * hidden, axis=1, keepdims=True)
        for i in range(n):
            spread = jnp.broadcast_to(product[i * ROWS:(i + 1) * ROWS], (ROWS, FS))
            placed = jnp.where(lane_of_slot(p + i), spread.reshape(PLANE, SLOT, FS), 0.0)
            pr[(p + i) // 4] += jnp.sum(placed, axis=1)
        gg = dh * u * sg * (1.0 + g * (1.0 - sg))
        ug = dh * act
        gx[0, rows, 0:FS] = gg.astype(BF16)
        gx[0, rows, FS:2 * FS] = ug.astype(BF16)
        for i, v in enumerate((gg, ug, hidden)):
            lo = jnp.where(first, v, 0.0).astype(BF16)
            hi = jnp.where(first, 0.0, v).astype(BF16)
            if i < 2:
                gu2[rows, 256 * i:256 * i + 128] = lo
                gu2[rows, 256 * i + 128:256 * i + 256] = hi
            else:
                h2[rows, 0:128] = lo
                h2[rows, 128:256] = hi

    @jax.named_scope("weight_grads")
    def weight_grads(k):
        at = pl.ds(pl.multiple_of(quarter(k) * Q, Q), Q)
        o = lax.dot_general(ts[k, 0], gu2[...], CONTRACT_MAJOR, preferred_element_type=F32)
        for i in range(2):
            dg[i, at, :] = o[:, i * FS:(i + 1) * FS]
            du[i, at, :] = o[:, 256 + i * FS:256 + (i + 1) * FS]
        o = lax.dot_general(h2[...], ts[k, 1], CONTRACT_MAJOR, preferred_element_type=F32)
        for i in range(2):
            dd[i, :, at] = o[i * FS:(i + 1) * FS]

    def rows_of(dz, lo=0, n=ROWS):
        return pl.ds(POS[dz] * ROWS + lo, n)

    def g_push(dz):
        r = rows_of(dz)
        push(gx.at[0, r], gx.at[1, r], g_s.at[0, dz], g_r.at[0, dz], at_x(1))
        push(gx.at[0, r], gx.at[2, r], g_s.at[1, dz], g_r.at[1, dz], at_x(NX - 1))

    @jax.named_scope("g_pass")
    def g_pass(dz):
        lo, hi = rows_of(dz, 0, 96), rows_of(dz, 96, 96)
        done(gx.at[1, rows_of(dz)], g_r.at[0, dz])
        push(gx.at[1, lo], gx.at[3, lo], gf_s.at[0, dz], gf_r.at[0, dz], at_x(1))
        done(gx.at[2, rows_of(dz)], g_r.at[1, dz])
        push(gx.at[2, hi], gx.at[3, hi], gf_s.at[1, dz], gf_r.at[1, dz], at_x(NX - 1))

    @jax.named_scope("ig_wait")
    def ig_wait(dz):
        done(gx.at[3, rows_of(dz, 0, 96)], gf_r.at[0, dz])
        done(gx.at[3, rows_of(dz, 96, 96)], gf_r.at[1, dz])

    @jax.named_scope("input_grad")
    def input_grad(dz):
        pos = POS[dz]
        first = first_of(1, FS)
        total = jnp.zeros((ROWS, Q), F32)
        for slot, w in ((0, None), (1, 0), (2, 2), (3, 1)):
            pair = gx[slot, rows_of(dz)].astype(F32)
            gg, ug = pair[:, 0:FS], pair[:, FS:2 * FS]
            lhs = jnp.concatenate(
                [
                    jnp.where(first, gg, 0.0).astype(BF16),
                    jnp.where(first, 0.0, gg).astype(BF16),
                    jnp.where(first, ug, 0.0).astype(BF16),
                    jnp.where(first, 0.0, ug).astype(BF16),
                ],
                axis=1,
            )
            rhs = wgu[x] if w is None else wq[w]
            total = total + lax.dot_general(lhs, rhs, CONTRACT_MINOR, preferred_element_type=F32)
        igs[pos] = total
        igr[pos, 0:SLOT] = total[0:SLOT]
        for j in range(1, PLANE):
            at = pl.ds(j * SLOT, SLOT)
            push(
                igs.at[pos, at], igr.at[pos, at], ig_s.at[pos], ig_r.at[pos], at_plane(j, -1),
                last=False,
            )
        sends.append((igs.at[pos, pl.ds(SLOT, ROWS - SLOT)], ig_s.at[pos]))

    @jax.named_scope("dense")
    def dense(dz):
        pos = POS[dz]
        with jax.named_scope("dense_wait"):
            done(igr.at[pos, pl.ds(SLOT, ROWS - SLOT)], ig_r.at[pos])
        pick = pk[pos]
        v = igr[pos]
        hi = v.astype(BF16)
        rest = v - hi.astype(F32)
        mid = rest.astype(BF16)
        low = (rest - mid.astype(F32)).astype(BF16)
        total = lax.dot_general(pick, hi, CONTRACT_MAJOR, preferred_element_type=F32)
        total = total + (
            lax.dot_general(pick, mid, CONTRACT_MAJOR, preferred_element_type=F32)
            + lax.dot_general(pick, low, CONTRACT_MAJOR, preferred_element_type=F32)
        )
        db[dz] = total

    @jax.named_scope("pair_products")
    def pair_products(dz):
        pos = POS[dz]
        row = lax.broadcasted_iota(I32, (ROWS, TOK), 0)
        slots = sl[pos, 0:2]
        spread = jnp.broadcast_to(prr[:, pos // 4][:, None, :], (PLANE, SLOT, FS))
        col = jnp.sum(
            jnp.where(lane_of_slot(pos), spread, 0.0).reshape(ROWS, FS), axis=1, keepdims=True
        )
        r0 = jnp.sum(jnp.where(row == slots[0:1], col, 0.0), axis=0, keepdims=True)
        r1 = jnp.sum(jnp.where(row == slots[1:2], col, 0.0), axis=0, keepdims=True)
        pb[dz] = jnp.concatenate([r0, r1, jnp.zeros((6, Q), F32)], axis=0)
        if dz:
            push(pb.at[dz], pe.at[dz], pz_s.at[dz], pz_r.at[dz], at_z(NZ - dz))

    def part(i):
        return pl.ds(PART * i, PART)

    @jax.named_scope("chain")
    def chain(dz, i):
        if dz < 4 or (dz == 4 and i < 2):
            land, at, dev = rm.at[dz - 1, part(i)], dz - 1, at_z(NZ - 1)
            if dz < 3 or (dz == 3 and i < 2):
                done(rm.at[dz, part(i)], c_r.at[i, dz])
                db[dz, part(i)] += rm[dz, part(i)]
        else:
            land, at, dev = rp.at[dz - 4, part(i)], dz, at_z(1)
            if dz > 5 or (dz == 5 and i >= 2):
                done(rp.at[dz - 5, part(i)], c_r.at[i, dz - 1])
                db[dz, part(i)] += rp[dz - 5, part(i)]
        push(db.at[dz, part(i)], land, c_s.at[i, dz], c_r.at[i, at], dev)

    for plus in (True, False):
        z_push(0, 0, plus)
        rb_push(0, plus)
    slots_of(0)
    for load in loads[4:10]:
        load.wait()
    for k in BRINGS[0]:
        build(0, k)
    with jax.named_scope("weights"):
        for q in range(4):
            for w in range(2):
                for i in range(2):
                    lane = 256 * w + FS * i
                    wgu[q, :, lane:lane + FS] = wv[w, i, q * Q:(q + 1) * Q, :]
        for s in range(1, NX):
            push(wgu.at[(x + s) % NX], wq.at[s - 1], w_s.at[s - 1], w_r.at[s - 1], at_x(s))
        for load in loads[10:]:
            load.wait()

    def take(blocks, k):
        for dz in blocks:
            z_take(dz, k)

    def make(blocks, k):
        for dz in blocks:
            if k == 0:
                slots_of(dz)
            build(dz, k)

    take((1, 7), 0)
    make((1, 7), 0)
    x_push(0)
    take((2, 6), 0)
    z_push(0, 3, True)
    z_push(0, 3, False)
    make((2, 6), 0)
    x_push(1)
    x_push(7)
    compute_wait(0)
    compute(0)
    x_push(2)
    x_push(6)
    take((3, 5), 0)
    make((3, 5), 0)
    take((1, 7), 3)
    make((1, 7), 3)
    x_push(3)
    x_push(5)
    take((4,), 0)
    make((4,), 0)
    x_push(4)
    take((2, 6), 3)
    make((2, 6), 3)
    z_push(0, 2, True)
    z_push(0, 1, False)
    compute_wait(2, 6)
    compute(2, 6)
    x_pass(4)
    g_push(2)
    take((3, 5), 3)
    make((3, 5), 3)
    compute_wait(4)
    compute(4)
    g_push(4)
    g_push(6)
    g_pass(2)
    z_take(1, 2)
    z_take(7, 1)
    build(1, 2)
    build(7, 1)
    compute_wait(3, 5)
    compute(3, 5)
    g_push(3)
    g_pass(4)
    with jax.named_scope("wq_wait"):
        for i in range(NX - 1):
            done(wq.at[i], w_r.at[i])

    def grad(dz):
        ig_wait(dz)
        input_grad(dz)

    g_push(5)
    g_pass(6)
    grad(2)
    grad(4)
    compute_wait(1, 7)
    compute(1, 7)
    g_push(1)

    for s in range(1, NX):
        push(pr, prx.at[s - 1], p_s.at[s - 1], p_r.at[s - 1], at_x(s))

    def products():
        with jax.named_scope("products"):
            for s in range(NX - 1):
                done(prx.at[s], p_r.at[s])
            total = pr[...] + prx[0] + prx[1] + prx[2]
            for j in range(PLANE):
                prs[j] = total[:, j]
            prr[0] = total[:, 0]
            for j in range(1, PLANE):
                push(prs.at[j], prr.at[j], pp_s, pp_r, at_plane(j, -1), last=False)
            sends.append((prs.at[pl.ds(1, PLANE - 1)], pp_s))

    outs = []

    def put(src, dst, sem):
        copy = pltpu.make_async_copy(src, dst, sem)
        copy.start()
        outs.append(copy)

    def early(dz):
        for i in (0, 1):
            chain(dz, 2 + i if dz < 4 else i)

    def later(dz):
        for i in (0, 1):
            chain(dz, i if dz < 4 else 2 + i)

    g_pass(3)
    g_push(7)
    grad(6)
    g_pass(5)
    g_push(0)
    dense(4)
    for i in range(4):
        chain(4, i)
    products()
    grad(3)
    dense(2)
    dense(6)
    g_pass(1)
    weight_grads(0)
    grad(5)
    dense(3)
    early(3)
    later(3)
    g_pass(7)
    with jax.named_scope("products_wait"):
        done(prr.at[pl.ds(1, PLANE - 1)], pp_r)
    for dz in (4, 3, 5):
        pair_products(dz)
    dense(5)
    early(5)
    later(5)
    g_pass(0)
    grad(1)
    weight_grads(1)
    early(2)
    grad(7)
    early(6)
    grad(0)
    later(2)
    dense(1)
    early(1)
    later(6)
    weight_grads(2)
    dense(7)
    early(7)
    weight_grads(3)
    put(dg, dg_out, out_s.at[0])
    put(du, du_out, out_s.at[1])
    put(dd, dd_out, out_s.at[2])
    dense(0)
    later(1)
    later(7)
    for dz in (2, 6, 1, 7, 0):
        pair_products(dz)
    with jax.named_scope("early_final"):
        for i in (0, 1):
            done(rm.at[0, part(2 + i)], c_r.at[2 + i, 0])
            db[0, part(2 + i)] += rm[0, part(2 + i)]
            done(rp.at[3, part(i)], c_r.at[i, 7])
            db[0, part(i)] += rp[3, part(i)]

    mine = pl.ds(pl.multiple_of(x * Q, Q), Q)
    with jax.named_scope("final"):
        for i in (0, 2, 1, 3):
            got, sem = (rm.at[0], c_r.at[i, 0]) if i < 2 else (rp.at[3], c_r.at[i, 7])
            done(got.at[part(i)], sem)
            tq[part(i)] = (db[0, part(i)] + got[part(i)]).astype(BF16)
            src, dst = tq.at[part(i)], tg_out.at[part(i), mine]
            for k in range(1, NX):
                push(src, dst, t_s.at[k - 1, i], t_r.at[k - 1, i], at_x(k))
        put(tq, tg_out.at[:, mine], out_s.at[3])
        total = pb[0]
        for dz in range(1, NZ):
            done(pe.at[dz], pz_r.at[dz])
            total = total + pe[dz]
        gg_out[...] = total[0:2] / gw[...]
    with jax.named_scope("gather"):
        for k in range(1, NX):
            theirs = pl.ds(pl.multiple_of((x + NX - k) % NX * Q, Q), Q)
            for i in range(4):
                done(tg_out.at[part(i), theirs], t_r.at[k - 1, i])
    with jax.named_scope("drain"):
        for src, sem in sends:
            done(src, sem)
        for copy in outs:
            copy.wait()


def carry(tg, gg, dg, du, dd, tg_out, gg_out, dg_out, du_out, dd_out, tg_v, w_v, d_v, in_s, out_s):
    pairs = [(tg, tg_v, tg_out)]
    for i, (a, b) in enumerate(((dg, dg_out), (du, du_out), (dd, dd_out))):
        for k in range(2):
            pairs.append((a.at[k], w_v.at[2 * i + k] if i < 2 else d_v.at[k], b.at[k]))
    views = []
    for i, (a, v, b) in enumerate(pairs):
        views.append((pltpu.make_async_copy(a, v, in_s.at[i]), pltpu.make_async_copy(v, b, out_s.at[i])))
    for load, _ in views:
        load.start()
    gg_out[...] = gg[...]
    for load, store in views:
        load.wait()
        store.start()
    for _, store in views:
        store.wait()


def shards(tokens, cotangent, routing, gate_weights, gate_proj, up_proj, down_proj):
    vmem = pl.BlockSpec(memory_space=pltpu.VMEM)
    hbm = pl.BlockSpec(memory_space=pl.ANY)
    dma = pltpu.SemaphoreType.DMA
    scratch = [
        pltpu.VMEM((len(HELD), 2, TOK, Q), BF16),
        pltpu.VMEM((NZ, 8, TOK), F32),
        pltpu.VMEM((len(BUILT), PLANE, 6, 8, Q), BF16),
        pltpu.VMEM((4, NZ, PLANE, 6, 8, Q), BF16),
        pltpu.VMEM((2, 2, D, FS), BF16),
        pltpu.VMEM((4, Q, 512), BF16),
        pltpu.VMEM((4, 256, Q), BF16),
        pltpu.VMEM((3, Q, 512), BF16),
        pltpu.VMEM((NZ, 8, TOK), I32),
        pltpu.VMEM((TOK, TOK), BF16),
        pltpu.VMEM((NZ, ROWS, TOK), BF16),
        pltpu.VMEM((NZ, ROWS, FS), F32),
        pltpu.VMEM((4, 2, ALL, Q), BF16),
        pltpu.VMEM((ALL, 512), BF16),
        pltpu.VMEM((ALL, 256), BF16),
        pltpu.VMEM((4, ALL, 256), BF16),
        pltpu.VMEM((2, PLANE, FS), F32),
        pltpu.VMEM((3, 2, PLANE, FS), F32),
        pltpu.VMEM((PLANE, 2, FS), F32),
        pltpu.VMEM((PLANE, 2, FS), F32),
        pltpu.VMEM((NZ, 8, Q), F32),
        pltpu.VMEM((NZ, 8, Q), F32),
        pltpu.VMEM((NZ, ROWS, Q), F32),
        pltpu.VMEM((NZ, ROWS, Q), F32),
        pltpu.VMEM((NZ, TOK, Q), F32),
        pltpu.VMEM((4, TOK, Q), F32),
        pltpu.VMEM((4, TOK, Q), F32),
        pltpu.VMEM((TOK, Q), BF16),
        pltpu.VMEM((2, D, FS), F32),
        pltpu.VMEM((2, D, FS), F32),
        pltpu.VMEM((2, FS, D), F32),
        dma((18,)), dma((2, len(HELD))), dma((2, len(HELD))), dma((2, 8)), dma((8,)),
        dma((len(BUILT),)), dma((len(BUILT),)),
        dma((2, 8)), dma((2, 8)), dma((2, 8)), dma((2, 8)),
        dma((3,)), dma((3,)), dma((2, 8)), dma((2, 8)), dma((2, 8)), dma((2, 8)),
        dma((3,)), dma((3,)), dma, dma, dma((8,)), dma((8,)), dma((8,)), dma((8,)),
        dma((4, 8)), dma((4, 8)), dma((3, 4)), dma((3, 4)), dma((7,)),
    ]
    tg, gg, dg, du, dd = pl.pallas_call(
        kernel,
        out_shape=(
            jax.ShapeDtypeStruct((TOK, D), BF16),
            jax.ShapeDtypeStruct((2, TOK), F32),
            jax.ShapeDtypeStruct((2, D, FS), F32),
            jax.ShapeDtypeStruct((2, D, FS), F32),
            jax.ShapeDtypeStruct((2, FS, D), F32),
        ),
        in_specs=[hbm, hbm, vmem, vmem, hbm, hbm, hbm],
        out_specs=(hbm, vmem, hbm, hbm, hbm),
        scratch_shapes=scratch,
        compiler_params=pltpu.CompilerParams(
            collective_id=0, has_side_effects=True, vmem_limit_bytes=63 * 1024 * 1024
        ),
    )(tokens, cotangent, routing.T, gate_weights.T, gate_proj, up_proj, down_proj)
    wide = jax.ShapeDtypeStruct((2, D, FS), F32)
    tg, gg, dg, du, dd = pl.pallas_call(
        carry,
        out_shape=(
            jax.ShapeDtypeStruct((TOK, D), BF16),
            jax.ShapeDtypeStruct((2, TOK), F32),
            wide, wide,
            jax.ShapeDtypeStruct((2, FS, D), F32),
        ),
        in_specs=[hbm, vmem, hbm, hbm, hbm],
        out_specs=(hbm, vmem, hbm, hbm, hbm),
        scratch_shapes=[
            pltpu.VMEM((TOK, D), BF16),
            pltpu.VMEM((4, D, FS), F32),
            pltpu.VMEM((2, FS, D), F32),
            dma((7,)),
            dma((7,)),
        ],
        compiler_params=pltpu.CompilerParams(vmem_limit_bytes=63 * 1024 * 1024),
    )(tg, gg, dg, du, dd)
    return tg, gg.T, dg, du, dd


def solution(mesh):
    in_specs = (
        P("ep", None),
        P("ep", None),
        P("ep", None),
        P("ep", None),
        P("ep", None, "tp"),
        P("ep", None, "tp"),
        P("ep", "tp", None),
    )
    out_specs = (
        P("ep", None),
        P("ep", None),
        P("ep", None, "tp"),
        P("ep", None, "tp"),
        P("ep", "tp", None),
    )
    return jax.shard_map(shards, mesh=mesh, in_specs=in_specs, out_specs=out_specs, check_vma=False)
```

```python
import jax
import jax.numpy as jnp
from jax import lax
from jax.experimental import pallas as pl
from jax.experimental.pallas import tpu as pltpu
from jax.sharding import PartitionSpec as P

F32 = jnp.float32
BF16 = jnp.bfloat16
I32 = jnp.int32
MESH = pl.DeviceIdType.MESH

NZ, NY, NC, NX = 8, 4, 2, 4
PLANE = NY * NC
TOK = 256
D = 1024
Q = 256
FS = 128
CAP = 12
SLOT = 2 * CAP
ROWS = PLANE * SLOT
ALL = NZ * ROWS
POS = {0: 0, 1: 1, 7: 2, 2: 3, 6: 4, 3: 5, 5: 6, 4: 7}
BRINGS = {
    0: (0, 3), 1: (0, 3, 2), 2: (0, 3), 3: (0, 3), 4: (0,), 5: (0, 3), 6: (0, 3), 7: (0, 3, 1),
}
HELD = [(0, k) for k in range(4)]
HELD += [(dz, k) for dz in (1, 2, 3, 5, 6, 7, 4) for k in BRINGS[dz]]
HELD = {key: i for i, key in enumerate(HELD)}
BUILT = {key: i for i, key in enumerate((dz, k) for dz in range(NZ) for k in BRINGS[dz])}
PART = TOK // 4
CONTRACT_MINOR = (((1,), (1,)), ((), ()))
CONTRACT_MAJOR = (((0,), (0,)), ((), ()))


def kernel(
    tok, cot, rt_in, gw_in, wg, wu, wd,
    tg_out, gg_out, dg_out, du_out, dd_out,
    rt, gw, gg, bk, rb, sx, rq, wv, wgu, wds, wq, sl, upper, pk, wt, ts, gu2, h2,
    gx, pr, prx, prs, prr, pb, pe, igs, igr, db, rm, rp, tq, dg, du, dd,
    in_s, z_s, z_r, rb_s, rb_r, ip_s, ip_r, x_s, x_r, xf_s, xf_r, w_s, w_r, g_s, g_r, gf_s, gf_r,
    p_s, p_r, pp_s, pp_r, pz_s, pz_r, ig_s, ig_r, c_s, c_r, t_s, t_r, out_s,
):
    e = lax.axis_index("ep")
    x = lax.axis_index("tp")
    z = e // PLANE
    y = (e % PLANE) // NC
    c = e % NC

    def at_z(step):
        return (((z + step) % NZ) * PLANE + y * NC + c, x)

    def at_plane(j, sign):
        dy, dc = j // NC, j % NC
        return (z * PLANE + ((y + sign * dy + NY) % NY) * NC + (c + dc) % NC, x)

    def at_x(step):
        return (e, (x + step) % NX)

    def remote(src, dst, ssem, rsem, dev):
        return pltpu.make_async_remote_copy(
            src_ref=src, dst_ref=dst, send_sem=ssem, recv_sem=rsem,
            device_id=dev, device_id_type=MESH,
        )

    def done(ref, sem):
        pltpu.make_async_copy(ref, ref, sem).wait()

    def push(src, dst, ssem, rsem, dev):
        remote(src, dst, ssem, rsem, dev).start()

    def quarter(k):
        who = (x + (0, NX - 1, 1, 2)[k]) % NX
        return 2 * (who % 2) + who // 2

    with jax.named_scope("prologue"):
        barrier = pltpu.get_barrier_semaphore()
        partners = [at_z(k) for k in range(1, NZ)]
        partners += [at_plane(j, 1) for j in range(1, PLANE)]
        partners += [at_x(s) for s in range(1, NX)]
        for dev in partners:
            pl.semaphore_signal(barrier, inc=1, device_id=dev, device_id_type=MESH)

        loads = [
            pltpu.make_async_copy(rt_in, rt, in_s.at[0]),
            pltpu.make_async_copy(gw_in, gw, in_s.at[1]),
        ]
        for k in (0, 3, 1, 2):
            cols = pl.ds(pl.multiple_of(quarter(k) * Q, Q), Q)
            dst = bk.at[HELD[0, k]]
            loads.append(pltpu.make_async_copy(tok.at[:, cols], dst.at[0], in_s.at[2 if k in (0, 3) else 3]))
            loads.append(pltpu.make_async_copy(cot.at[:, cols], dst.at[1], in_s.at[2 if k in (0, 3) else 3]))
        for i, w in enumerate((wg, wu)):
            loads.append(pltpu.make_async_copy(w, wv.at[i], in_s.at[4]))
        for q in range(4):
            for i in range(2):
                loads.append(
                    pltpu.make_async_copy(
                        wd.at[i, :, pl.ds(q * Q, Q)], wds.at[q, pl.ds(i * FS, FS)], in_s.at[5]
                    )
                )
        for load in loads:
            load.start()
        upper[...] = (
            lax.broadcasted_iota(I32, (TOK, TOK), 0) < lax.broadcasted_iota(I32, (TOK, TOK), 1)
        ).astype(F32).astype(BF16)
        pr[...] = jnp.zeros_like(pr)
        loads[0].wait()
        loads[1].wait()
        done(bk.at[pl.ds(0, 2)], in_s.at[2])
        rb[0] = jnp.concatenate(
            [rt[...].astype(F32), gw[...], jnp.zeros((4, TOK), F32)], axis=0
        )
    with jax.named_scope("barrier"):
        pl.semaphore_wait(barrier, len(partners))

    def first_of(n, lanes):
        i = lax.broadcasted_iota(I32, (n * PLANE, SLOT, lanes), 1)
        return (i < CAP).reshape(n * ROWS, lanes)

    def lane_of_slot(pos):
        i = lax.broadcasted_iota(I32, (PLANE, SLOT, FS), 1)
        l = lax.broadcasted_iota(I32, (PLANE, SLOT, FS), 2)
        return i + 32 * (pos % 4) == l

    def toward(dz, plus):
        return (dz + 1, at_z(1)) if plus else ((dz + NZ - 1) % NZ, at_z(NZ - 1))

    def z_push(dz, k, plus):
        to, dev = toward(dz, plus)
        src, i = bk.at[HELD[dz, k]], HELD[to, k]
        if to == 4:
            a = 0 if plus else 1
            push(src.at[a], bk.at[i, a], z_s, z_r.at[i + a], dev)
        else:
            push(src, bk.at[i], z_s, z_r.at[i], dev)

    @jax.named_scope("z_take")
    def z_take(dz, k, onward=True):
        i = HELD[dz, k]
        plus = dz < 4
        first = k == 0
        if first:
            done(rb.at[dz], rb_r.at[dz])
            if dz < 4 or dz > 5:
                if dz != 4:
                    rb_push(dz, plus)
        if dz == 4:
            for a in range(2):
                done(bk.at[i, a], z_r.at[i + a])
            return
        done(bk.at[i], z_r.at[i])
        if k in BRINGS[toward(dz, plus)[0]]:
            z_push(dz, k, plus)

    def rb_push(dz, plus):
        if plus:
            to, dev, i = dz + 1, at_z(1), 0
        else:
            to, dev, i = (dz + NZ - 1) % NZ, at_z(NZ - 1), 1
        push(rb.at[dz], rb.at[to], rb_s, rb_r.at[to], dev)

    @jax.named_scope("slots_of")
    def slots_of(dz):
        pos = POS[dz]
        e16 = lax.broadcasted_iota(I32, (16, TOK), 0)
        target = ((e16 // 4 - y) & 3) * NC + (((e16 // 2) - c) & 1)
        base = (target * SLOT + (e16 & 1) * CAP).astype(F32)
        block = rb[dz]
        chosen = block[0:2].astype(I32) - z * 16
        e0 = (e16 == chosen[0:1]).astype(F32)
        e1 = (e16 == chosen[1:2]).astype(F32)
        both = jnp.concatenate([e0, e1], axis=0).astype(BF16)
        before = jnp.dot(both, upper[...], preferred_element_type=F32)
        before0 = before[0:16]
        before1 = before[16:32] + jnp.sum(e0, axis=1, keepdims=True)
        s0 = jnp.sum(e0 * (base + before0 + 1.0), axis=0, keepdims=True) - 1.0
        s1 = jnp.sum(e1 * (base + before1 + 1.0), axis=0, keepdims=True) - 1.0
        slots = jnp.concatenate([s0, s1], axis=0).astype(I32)
        sl[pos, 0:2] = slots
        row = lax.broadcasted_iota(I32, (ROWS, TOK), 0)
        p0 = row == slots[0:1]
        p1 = row == slots[1:2]
        pk[pos] = (p0 | p1).astype(F32).astype(BF16)
        weight = jnp.sum(
            jnp.where(p0, block[2:3], 0.0) + jnp.where(p1, block[3:4], 0.0),
            axis=1, keepdims=True,
        )
        wt[pos] = jnp.broadcast_to(weight, (ROWS, FS))

    @jax.named_scope("build")
    def build(dz, k):
        pos, b = POS[dz], BUILT[dz, k]
        src, stage, land = bk.at[HELD[dz, k]], sx.at[b], rq.at[k, pos]
        pick = pk[pos]
        w = jnp.concatenate([wt[pos], wt[pos]], axis=1)
        t = jnp.dot(pick, src[0], preferred_element_type=F32)
        s = jnp.dot(pick, src[1], preferred_element_type=F32) * w
        t = t.reshape(PLANE, 3, 8, Q).astype(BF16)
        s = s.reshape(PLANE, 3, 8, Q).astype(BF16)
        stage[:, 0:3] = t
        stage[:, 3:6] = s
        land[0, 0:3] = t[0]
        land[0, 3:6] = s[0]
        for j in range(1, PLANE):
            push(stage.at[j], land.at[j], ip_s, ip_r.at[b], at_plane(j, 1))

    def landed(dz, k):
        done(rq.at[k, POS[dz], pl.ds(1, PLANE - 1)], ip_r.at[BUILT[dz, k]])

    @jax.named_scope("x_push")
    def x_push(dz):
        pos = POS[dz]
        landed(dz, 0)
        if 1 not in BRINGS[dz]:
            push(rq.at[0, pos], rq.at[1, pos], x_s, x_r.at[0, pos], at_x(1))
        if 2 not in BRINGS[dz]:
            push(rq.at[0, pos], rq.at[2, pos], x_s, x_r.at[1, pos], at_x(NX - 1))

    low, high = pl.ds(0, PLANE // 2), pl.ds(PLANE // 2, PLANE // 2)

    @jax.named_scope("x_pass")
    def x_pass(dz):
        pos = POS[dz]
        done(rq.at[1, pos], x_r.at[0, pos])
        push(rq.at[1, pos, low], rq.at[3, pos, low], xf_s, xf_r.at[0], at_x(1))
        done(rq.at[2, pos], x_r.at[1, pos])
        push(
            rq.at[2, pos, high], rq.at[3, pos, high], xf_s, xf_r.at[1],
            at_x(NX - 1),
        )

    @jax.named_scope("compute_wait")
    def compute_wait(*blocks):
        for dz in blocks:
            pos, own = POS[dz], BRINGS[dz]
            for k in own[1:]:
                landed(dz, k)
            if 3 not in own:
                done(rq.at[3, pos, low], xf_r.at[0])
                done(rq.at[3, pos, high], xf_r.at[1])
            else:
                for k in (1, 2):
                    if k not in own:
                        done(rq.at[k, pos], x_r.at[k - 1, pos])

    @jax.named_scope("compute")
    def compute(*blocks):
        p, n = POS[blocks[0]], len(blocks)
        m = n * ROWS
        rows = pl.ds(p * ROWS, m)
        pre = jnp.zeros((m, 512), F32)
        hg = jnp.zeros((m, 256), F32)
        for k in range(4):
            src = rq.at[k]
            t = src[p:p + n, :, 0:3].astype(F32).reshape(m, Q).astype(BF16)
            s = src[p:p + n, :, 3:6].astype(F32).reshape(m, Q).astype(BF16)
            ts[k, 0, rows] = t
            ts[k, 1, rows] = s
            pre = pre + jnp.dot(t, wgu[quarter(k)], preferred_element_type=F32)
            hg = hg + lax.dot_general(
                s, wds[quarter(k)], CONTRACT_MINOR, preferred_element_type=F32
            )
        first = first_of(n, FS)
        g = jnp.where(first, pre[:, 0:128], pre[:, 128:256]).astype(BF16).astype(F32)
        u = jnp.where(first, pre[:, 256:384], pre[:, 384:512]).astype(BF16).astype(F32)
        dh = jnp.where(first, hg[:, 0:128], hg[:, 128:256])
        sg = jax.nn.sigmoid(g)
        act = g * sg
        hidden = act * u
        product = jnp.sum(dh * hidden, axis=1, keepdims=True)
        for i in range(n):
            spread = jnp.broadcast_to(product[i * ROWS:(i + 1) * ROWS], (ROWS, FS))
            placed = jnp.where(lane_of_slot(p + i), spread.reshape(PLANE, SLOT, FS), 0.0)
            pr[(p + i) // 4] += jnp.sum(placed, axis=1)
        gg = dh * u * sg * (1.0 + g * (1.0 - sg))
        ug = dh * act
        gx[0, rows, 0:FS] = gg.astype(BF16)
        gx[0, rows, FS:2 * FS] = ug.astype(BF16)
        for i, v in enumerate((gg, ug, hidden)):
            lo = jnp.where(first, v, 0.0).astype(BF16)
            hi = jnp.where(first, 0.0, v).astype(BF16)
            if i < 2:
                gu2[rows, 256 * i:256 * i + 128] = lo
                gu2[rows, 256 * i + 128:256 * i + 256] = hi
            else:
                h2[rows, 0:128] = lo
                h2[rows, 128:256] = hi

    @jax.named_scope("weight_grads")
    def weight_grads(k):
        at = pl.ds(pl.multiple_of(quarter(k) * Q, Q), Q)
        o = lax.dot_general(ts[k, 0], gu2[...], CONTRACT_MAJOR, preferred_element_type=F32)
        for i in range(2):
            dg[i, at, :] = o[:, i * FS:(i + 1) * FS]
            du[i, at, :] = o[:, 256 + i * FS:256 + (i + 1) * FS]
        o = lax.dot_general(h2[...], ts[k, 1], CONTRACT_MAJOR, preferred_element_type=F32)
        for i in range(2):
            dd[i, :, at] = o[i * FS:(i + 1) * FS]

    def rows_of(dz, lo=0, n=ROWS):
        return pl.ds(POS[dz] * ROWS + lo, n)

    def g_push(dz):
        r = rows_of(dz)
        push(gx.at[0, r], gx.at[1, r], g_s, g_r.at[0, dz], at_x(1))
        push(gx.at[0, r], gx.at[2, r], g_s, g_r.at[1, dz], at_x(NX - 1))

    @jax.named_scope("g_pass")
    def g_pass(dz):
        lo, hi = rows_of(dz, 0, 96), rows_of(dz, 96, 96)
        done(gx.at[1, rows_of(dz)], g_r.at[0, dz])
        push(gx.at[1, lo], gx.at[3, lo], gf_s, gf_r.at[0, dz], at_x(1))
        done(gx.at[2, rows_of(dz)], g_r.at[1, dz])
        push(gx.at[2, hi], gx.at[3, hi], gf_s, gf_r.at[1, dz], at_x(NX - 1))

    @jax.named_scope("ig_wait")
    def ig_wait(dz):
        done(gx.at[3, rows_of(dz, 0, 96)], gf_r.at[0, dz])
        done(gx.at[3, rows_of(dz, 96, 96)], gf_r.at[1, dz])

    @jax.named_scope("input_grad")
    def input_grad(dz):
        pos = POS[dz]
        first = first_of(1, FS)
        total = jnp.zeros((ROWS, Q), F32)
        for slot, w in ((0, None), (1, 0), (2, 2), (3, 1)):
            pair = gx[slot, rows_of(dz)].astype(F32)
            gg, ug = pair[:, 0:FS], pair[:, FS:2 * FS]
            lhs = jnp.concatenate(
                [
                    jnp.where(first, gg, 0.0).astype(BF16),
                    jnp.where(first, 0.0, gg).astype(BF16),
                    jnp.where(first, ug, 0.0).astype(BF16),
                    jnp.where(first, 0.0, ug).astype(BF16),
                ],
                axis=1,
            )
            rhs = wgu[x] if w is None else wq[w]
            total = total + lax.dot_general(lhs, rhs, CONTRACT_MINOR, preferred_element_type=F32)
        igs[pos] = total
        igr[pos, 0:SLOT] = total[0:SLOT]
        for j in range(1, PLANE):
            at = pl.ds(j * SLOT, SLOT)
            push(
                igs.at[pos, at], igr.at[pos, at], ig_s, ig_r.at[pos], at_plane(j, -1),
            )

    @jax.named_scope("dense")
    def dense(dz):
        pos = POS[dz]
        with jax.named_scope("dense_wait"):
            done(igr.at[pos, pl.ds(SLOT, ROWS - SLOT)], ig_r.at[pos])
        pick = pk[pos]
        v = igr[pos]
        hi = v.astype(BF16)
        rest = v - hi.astype(F32)
        mid = rest.astype(BF16)
        low = (rest - mid.astype(F32)).astype(BF16)
        total = lax.dot_general(pick, hi, CONTRACT_MAJOR, preferred_element_type=F32)
        total = total + (
            lax.dot_general(pick, mid, CONTRACT_MAJOR, preferred_element_type=F32)
            + lax.dot_general(pick, low, CONTRACT_MAJOR, preferred_element_type=F32)
        )
        db[dz] = total

    @jax.named_scope("pair_products")
    def pair_products(dz):
        pos = POS[dz]
        row = lax.broadcasted_iota(I32, (ROWS, TOK), 0)
        slots = sl[pos, 0:2]
        spread = jnp.broadcast_to(prr[:, pos // 4][:, None, :], (PLANE, SLOT, FS))
        col = jnp.sum(
            jnp.where(lane_of_slot(pos), spread, 0.0).reshape(ROWS, FS), axis=1, keepdims=True
        )
        r0 = jnp.sum(jnp.where(row == slots[0:1], col, 0.0), axis=0, keepdims=True)
        r1 = jnp.sum(jnp.where(row == slots[1:2], col, 0.0), axis=0, keepdims=True)
        pb[dz] = jnp.concatenate([r0, r1, jnp.zeros((6, Q), F32)], axis=0)
        if dz:
            push(pb.at[dz], pe.at[dz], pz_s, pz_r, at_z(NZ - dz))

    def part(i):
        return pl.ds(PART * i, PART)

    @jax.named_scope("chain")
    def chain(dz, i):
        if dz < 4 or (dz == 4 and i < 2):
            land, at, dev = rm.at[dz - 1, part(i)], dz - 1, at_z(NZ - 1)
            if dz < 3 or (dz == 3 and i < 2):
                done(rm.at[dz, part(i)], c_r.at[i, dz])
                db[dz, part(i)] += rm[dz, part(i)]
        else:
            land, at, dev = rp.at[dz - 4, part(i)], dz, at_z(1)
            if dz > 5 or (dz == 5 and i >= 2):
                done(rp.at[dz - 5, part(i)], c_r.at[i, dz - 1])
                db[dz, part(i)] += rp[dz - 5, part(i)]
        push(db.at[dz, part(i)], land, c_s, c_r.at[i, at], dev)

    def products():
        with jax.named_scope("products"):
            done(prx, p_r)
            total = pr[...] + prx[0] + prx[1] + prx[2]
            for j in range(PLANE):
                prs[j] = total[:, j]
            prr[0] = total[:, 0]
            for j in range(1, PLANE):
                push(prs.at[j], prr.at[j], pp_s, pp_r, at_plane(j, -1))

    def put(src, dst, sem):
        pltpu.make_async_copy(src, dst, sem).start()

    def early(dz):
        for i in (0, 1):
            chain(dz, 2 + i if dz < 4 else i)

    def later(dz):
        for i in (0, 1):
            chain(dz, i if dz < 4 else 2 + i)

    def grad(dz):
        ig_wait(dz)
        input_grad(dz)

    for plus in (True, False):
        z_push(0, 0, plus)
        rb_push(0, plus)
    slots_of(0)
    done(bk.at[pl.ds(0, 2)], in_s.at[3])
    done(wv, in_s.at[4])
    for k in BRINGS[0]:
        build(0, k)
    with jax.named_scope("weights"):
        for q in range(4):
            for w in range(2):
                for i in range(2):
                    lane = 256 * w + FS * i
                    wgu[q, :, lane:lane + FS] = wv[w, i, q * Q:(q + 1) * Q, :]
        for s in range(1, NX):
            push(wgu.at[(x + s) % NX], wq.at[s - 1], w_s, w_r, at_x(s))
        done(wds, in_s.at[5])

    def take(blocks, k):
        for dz in blocks:
            z_take(dz, k)

    def make(blocks, k):
        for dz in blocks:
            if k == 0:
                slots_of(dz)
            build(dz, k)

    take((1, 7), 0)
    make((1, 7), 0)
    x_push(0)
    take((2, 6), 0)
    z_push(0, 3, True)
    z_push(0, 3, False)
    make((2, 6), 0)
    x_push(1)
    x_push(7)
    compute_wait(0)
    compute(0)
    x_push(2)
    x_push(6)
    take((3, 5), 0)
    make((3, 5), 0)
    take((1, 7), 3)
    make((1, 7), 3)
    x_push(3)
    x_push(5)
    take((4,), 0)
    make((4,), 0)
    x_push(4)
    take((2, 6), 3)
    make((2, 6), 3)
    z_push(0, 2, True)
    z_push(0, 1, False)
    compute_wait(2, 6)
    compute(2, 6)
    x_pass(4)
    g_push(2)
    g_push(6)
    take((3, 5), 3)
    make((3, 5), 3)
    z_take(1, 2)
    z_take(7, 1)
    build(1, 2)
    build(7, 1)
    g_pass(2)
    compute_wait(4)
    compute(4)
    g_push(4)
    compute_wait(3, 5)
    compute(3, 5)
    g_pass(6)
    g_push(3)
    with jax.named_scope("wq_wait"):
        done(wq, w_r)
    grad(2)
    g_pass(4)
    g_push(5)
    grad(6)
    compute_wait(1, 7)
    compute(1, 7)

    for s in range(1, NX):
        push(pr, prx.at[s - 1], p_s, p_r, at_x(s))
    g_pass(3)
    g_push(1)
    grad(4)
    g_pass(5)
    g_push(7)
    dense(2)
    dense(6)
    grad(3)
    products()
    g_pass(1)
    g_push(0)
    dense(4)
    for i in range(4):
        chain(4, i)
    grad(5)
    dense(3)
    early(3)
    g_pass(7)
    later(3)
    grad(1)
    dense(5)
    early(5)
    later(5)
    g_pass(0)
    early(2)
    grad(7)
    later(2)
    early(6)
    dense(1)
    early(1)
    later(6)
    grad(0)
    later(1)
    dense(7)
    early(7)
    later(7)
    with jax.named_scope("products_wait"):
        done(prr.at[pl.ds(1, PLANE - 1)], pp_r)
    for dz in (4, 3, 5, 2, 6, 1, 7, 0):
        pair_products(dz)
    dense(0)
    with jax.named_scope("early_final"):
        for i in (0, 1):
            done(rm.at[0, part(2 + i)], c_r.at[2 + i, 0])
            db[0, part(2 + i)] += rm[0, part(2 + i)]
            done(rp.at[3, part(i)], c_r.at[i, 7])
            db[0, part(i)] += rp[3, part(i)]

    mine = pl.ds(pl.multiple_of(x * Q, Q), Q)
    with jax.named_scope("final"):
        for i in (0, 2, 1, 3):
            got, sem = (rm.at[0], c_r.at[i, 0]) if i < 2 else (rp.at[3], c_r.at[i, 7])
            done(got.at[part(i)], sem)
            tq[part(i)] = (db[0, part(i)] + got[part(i)]).astype(BF16)
            src, dst = tq.at[part(i)], tg_out.at[part(i), mine]
            for k in range(1, NX):
                push(src, dst, t_s, t_r, at_x(k))
        put(tq, tg_out.at[:, mine], out_s.at[0])
    for k in range(4):
        weight_grads(k)
        at = pl.ds(pl.multiple_of(quarter(k) * Q, Q), Q)
        put(dg.at[:, at], dg_out.at[:, at], out_s.at[1])
        put(du.at[:, at], du_out.at[:, at], out_s.at[2])
        put(dd.at[:, :, at], dd_out.at[:, :, at], out_s.at[3])
    done(pe.at[pl.ds(1, NZ - 1)], pz_r)
    total = pb[0]
    for dz in range(1, NZ):
        total = total + pe[dz]
    gg[...] = total[0:2] / gw[...]
    put(gg, gg_out, out_s.at[4])
    with jax.named_scope("gather"):
        done(gx.at[0, pl.ds(0, 3 * TOK)], t_r)
    with jax.named_scope("drain"):
        done(bk.at[pl.ds(0, 15)], z_s)
        done(rb.at[pl.ds(0, 7)], rb_s)
        done(sx.at[:, pl.ds(1, PLANE - 1)], ip_s)
        done(rq.at[pl.ds(0, 2), pl.ds(0, 7)], x_s)
        done(rq.at[0, 0], xf_s)
        done(wq, w_s)
        done(gx.at[pl.ds(0, 2)], g_s)
        done(gx.at[0], gf_s)
        done(prx, p_s)
        done(prs.at[pl.ds(1, PLANE - 1)], pp_s)
        done(pb.at[pl.ds(0, NZ - 1)], pz_s)
        done(igs.at[:, pl.ds(SLOT, ROWS - SLOT)], ig_s)
        done(db.at[pl.ds(0, 7)], c_s)
        done(gx.at[0, pl.ds(0, 3 * TOK)], t_s)
        done(tq, out_s.at[0])
        done(dg, out_s.at[1])
        done(du, out_s.at[2])
        done(dd, out_s.at[3])
        done(gg, out_s.at[4])


def carry(tg, gg, dg, du, dd, tg_out, gg_out, dg_out, du_out, dd_out, tg_v, gg_v, w_v, d_v, in_s, out_s):
    pairs = [(tg, tg_v, tg_out), (gg, gg_v, gg_out)]
    for i, (a, b) in enumerate(((dg, dg_out), (du, du_out), (dd, dd_out))):
        for k in range(2):
            pairs.append((a.at[k], w_v.at[2 * i + k] if i < 2 else d_v.at[k], b.at[k]))
    views = []
    for i, (a, v, b) in enumerate(pairs):
        views.append((pltpu.make_async_copy(a, v, in_s.at[i]), pltpu.make_async_copy(v, b, out_s.at[i])))
    for load, _ in views:
        load.start()
    for load, store in views:
        load.wait()
        store.start()
    for _, store in views:
        store.wait()


def shards(tokens, cotangent, routing, gate_weights, gate_proj, up_proj, down_proj):
    hbm = pl.BlockSpec(memory_space=pl.ANY)
    dma = pltpu.SemaphoreType.DMA
    scratch = [
        pltpu.VMEM((2, TOK), I32),
        pltpu.VMEM((2, TOK), F32),
        pltpu.VMEM((2, TOK), F32),
        pltpu.VMEM((len(HELD), 2, TOK, Q), BF16),
        pltpu.VMEM((NZ, 8, TOK), F32),
        pltpu.VMEM((len(BUILT), PLANE, 6, 8, Q), BF16),
        pltpu.VMEM((4, NZ, PLANE, 6, 8, Q), BF16),
        pltpu.VMEM((2, 2, D, FS), BF16),
        pltpu.VMEM((4, Q, 512), BF16),
        pltpu.VMEM((4, 256, Q), BF16),
        pltpu.VMEM((3, Q, 512), BF16),
        pltpu.VMEM((NZ, 8, TOK), I32),
        pltpu.VMEM((TOK, TOK), BF16),
        pltpu.VMEM((NZ, ROWS, TOK), BF16),
        pltpu.VMEM((NZ, ROWS, FS), F32),
        pltpu.VMEM((4, 2, ALL, Q), BF16),
        pltpu.VMEM((ALL, 512), BF16),
        pltpu.VMEM((ALL, 256), BF16),
        pltpu.VMEM((4, ALL, 256), BF16),
        pltpu.VMEM((2, PLANE, FS), F32),
        pltpu.VMEM((3, 2, PLANE, FS), F32),
        pltpu.VMEM((PLANE, 2, FS), F32),
        pltpu.VMEM((PLANE, 2, FS), F32),
        pltpu.VMEM((NZ, 8, Q), F32),
        pltpu.VMEM((NZ, 8, Q), F32),
        pltpu.VMEM((NZ, ROWS, Q), F32),
        pltpu.VMEM((NZ, ROWS, Q), F32),
        pltpu.VMEM((NZ, TOK, Q), F32),
        pltpu.VMEM((4, TOK, Q), F32),
        pltpu.VMEM((4, TOK, Q), F32),
        pltpu.VMEM((TOK, Q), BF16),
        pltpu.VMEM((2, D, FS), F32),
        pltpu.VMEM((2, D, FS), F32),
        pltpu.VMEM((2, FS, D), F32),
        dma((6,)), dma, dma((len(HELD) + 1,)), dma, dma((8,)),
        dma, dma((len(BUILT),)),
        dma, dma((2, 8)), dma, dma((2,)),
        dma, dma, dma, dma((2, 8)), dma, dma((2, 8)),
        dma, dma, dma, dma, dma, dma, dma, dma((8,)),
        dma, dma((4, 8)), dma, dma, dma((5,)),
    ]
    tg, gg, dg, du, dd = pl.pallas_call(
        kernel,
        out_shape=(
            jax.ShapeDtypeStruct((TOK, D), BF16),
            jax.ShapeDtypeStruct((2, TOK), F32),
            jax.ShapeDtypeStruct((2, D, FS), F32),
            jax.ShapeDtypeStruct((2, D, FS), F32),
            jax.ShapeDtypeStruct((2, FS, D), F32),
        ),
        in_specs=[hbm] * 7,
        out_specs=(hbm,) * 5,
        scratch_shapes=scratch,
        compiler_params=pltpu.CompilerParams(
            collective_id=0, has_side_effects=True, vmem_limit_bytes=63 * 1024 * 1024
        ),
    )(tokens, cotangent, routing.T, gate_weights.T, gate_proj, up_proj, down_proj)
    wide = jax.ShapeDtypeStruct((2, D, FS), F32)
    tg, gg, dg, du, dd = pl.pallas_call(
        carry,
        out_shape=(
            jax.ShapeDtypeStruct((TOK, D), BF16),
            jax.ShapeDtypeStruct((2, TOK), F32),
            wide, wide,
            jax.ShapeDtypeStruct((2, FS, D), F32),
        ),
        in_specs=[hbm] * 5,
        out_specs=(hbm,) * 5,
        scratch_shapes=[
            pltpu.VMEM((TOK, D), BF16),
            pltpu.VMEM((2, TOK), F32),
            pltpu.VMEM((4, D, FS), F32),
            pltpu.VMEM((2, FS, D), F32),
            dma((8,)),
            dma((8,)),
        ],
        compiler_params=pltpu.CompilerParams(vmem_limit_bytes=63 * 1024 * 1024),
    )(tg, gg, dg, du, dd)
    return tg, gg.T, dg, du, dd


def solution(mesh):
    in_specs = (
        P("ep", None),
        P("ep", None),
        P("ep", None),
        P("ep", None),
        P("ep", None, "tp"),
        P("ep", None, "tp"),
        P("ep", "tp", None),
    )
    out_specs = (
        P("ep", None),
        P("ep", None),
        P("ep", None, "tp"),
        P("ep", None, "tp"),
        P("ep", "tp", None),
    )
    return jax.shard_map(shards, mesh=mesh, in_specs=in_specs, out_specs=out_specs, check_vma=False)
```

```python
import jax
import jax.numpy as jnp
from jax import lax
from jax.experimental import pallas as pl
from jax.experimental.pallas import tpu as pltpu
from jax.sharding import PartitionSpec as P

F32 = jnp.float32
BF16 = jnp.bfloat16
I32 = jnp.int32
MESH = pl.DeviceIdType.MESH

NZ, NY, NC, NX = 8, 4, 2, 4
PLANE = NY * NC
TOK = 256
D = 1024
Q = 256
FS = 128
CAP = 12
SLOT = 2 * CAP
ROWS = PLANE * SLOT
ALL = NZ * ROWS
POS = {0: 0, 1: 1, 7: 2, 2: 3, 6: 4, 3: 5, 5: 6, 4: 7}
BRINGS = {
    0: (0, 3), 1: (0, 3, 2), 2: (0, 3), 3: (0, 3), 4: (0,), 5: (0, 3), 6: (0, 3), 7: (0, 3, 1),
}
HELD = [(0, k) for k in range(4)]
HELD += [(dz, k) for dz in (1, 2, 3, 5, 6, 7, 4) for k in BRINGS[dz]]
HELD = {key: i for i, key in enumerate(HELD)}
BUILT = {key: i for i, key in enumerate((dz, k) for dz in range(NZ) for k in BRINGS[dz])}
PART = TOK // 4
CONTRACT_MINOR = (((1,), (1,)), ((), ()))
CONTRACT_MAJOR = (((0,), (0,)), ((), ()))


def kernel(
    tok, cot, rt_in, gw_in, wg, wu, wd,
    tg_out, gg_out, dg_out, du_out, dd_out,
    rt, gw, gg, bk, rb, sx, rq, wv, wgu, wds, wq, sl, upper, pk, wt, ts, gu2, h2,
    gx, pr, prx, prs, prr, pb, pe, igs, igr, db, rm, rp, tq, dg, du, dd,
    in_s, z_s, z_r, rb_s, rb_r, ip_s, ip_r, x_s, x_r, xf_s, xf_r, w_s, w_r, g_s, g_r, gf_s, gf_r,
    p_s, p_r, pp_s, pp_r, pz_s, pz_r, ig_s, ig_r, c_s, c_r, t_s, t_r, out_s,
):
    e = lax.axis_index("ep")
    x = lax.axis_index("tp")
    z = e // PLANE
    y = (e % PLANE) // NC
    c = e % NC

    def at_z(step):
        return (((z + step) % NZ) * PLANE + y * NC + c, x)

    def at_plane(j, sign):
        dy, dc = j // NC, j % NC
        return (z * PLANE + ((y + sign * dy + NY) % NY) * NC + (c + dc) % NC, x)

    def at_x(step):
        return (e, (x + step) % NX)

    def remote(src, dst, ssem, rsem, dev):
        return pltpu.make_async_remote_copy(
            src_ref=src, dst_ref=dst, send_sem=ssem, recv_sem=rsem,
            device_id=dev, device_id_type=MESH,
        )

    def done(ref, sem):
        pltpu.make_async_copy(ref, ref, sem).wait()

    def push(src, dst, ssem, rsem, dev):
        remote(src, dst, ssem, rsem, dev).start()

    def quarter(k):
        who = (x + (0, NX - 1, 1, 2)[k]) % NX
        return 2 * (who % 2) + who // 2

    with jax.named_scope("prologue"):
        barrier = pltpu.get_barrier_semaphore()
        partners = [at_z(k) for k in range(1, NZ)]
        partners += [at_plane(j, 1) for j in range(1, PLANE)]
        partners += [at_x(s) for s in range(1, NX)]
        for dev in partners:
            pl.semaphore_signal(barrier, inc=1, device_id=dev, device_id_type=MESH)

        loads = [
            pltpu.make_async_copy(rt_in, rt, in_s.at[0]),
            pltpu.make_async_copy(gw_in, gw, in_s.at[1]),
        ]
        for k in (0, 3, 1, 2):
            cols = pl.ds(pl.multiple_of(quarter(k) * Q, Q), Q)
            dst = bk.at[HELD[0, k]]
            loads.append(pltpu.make_async_copy(tok.at[:, cols], dst.at[0], in_s.at[2 if k in (0, 3) else 3]))
            loads.append(pltpu.make_async_copy(cot.at[:, cols], dst.at[1], in_s.at[2 if k in (0, 3) else 3]))
        for i, w in enumerate((wg, wu)):
            loads.append(pltpu.make_async_copy(w, wv.at[i], in_s.at[4]))
        for q in range(4):
            for i in range(2):
                loads.append(
                    pltpu.make_async_copy(
                        wd.at[i, :, pl.ds(q * Q, Q)], wds.at[q, pl.ds(i * FS, FS)], in_s.at[5]
                    )
                )
        for load in loads:
            load.start()
        upper[...] = (
            lax.broadcasted_iota(I32, (TOK, TOK), 0) < lax.broadcasted_iota(I32, (TOK, TOK), 1)
        ).astype(F32).astype(BF16)
        pr[...] = jnp.zeros_like(pr)
        loads[0].wait()
        loads[1].wait()
        done(bk.at[pl.ds(0, 2)], in_s.at[2])
        rb[0] = jnp.concatenate(
            [rt[...].astype(F32), gw[...], jnp.zeros((4, TOK), F32)], axis=0
        )
    with jax.named_scope("barrier"):
        pl.semaphore_wait(barrier, len(partners))

    def first_of(n, lanes):
        i = lax.broadcasted_iota(I32, (n * PLANE, SLOT, lanes), 1)
        return (i < CAP).reshape(n * ROWS, lanes)

    def lane_of_slot(pos):
        i = lax.broadcasted_iota(I32, (PLANE, SLOT, FS), 1)
        l = lax.broadcasted_iota(I32, (PLANE, SLOT, FS), 2)
        return i + 32 * (pos % 4) == l

    def toward(dz, plus):
        return (dz + 1, at_z(1)) if plus else ((dz + NZ - 1) % NZ, at_z(NZ - 1))

    count = {"z": 0, "x": 0}

    def z_push(dz, k, plus, a):
        to, dev = toward(dz, plus)
        i = HELD[to, k]
        count["z"] += 1
        push(bk.at[HELD[dz, k], a], bk.at[i, a], z_s, z_r.at[i, a], dev)

    def z_own(k):
        for step in range(2):
            z_push(0, k, True, step)
            z_push(0, k, False, 1 - step)

    @jax.named_scope("z_take")
    def z_take(dz, k, step):
        for near in (dz, NZ - dz):
            plus = near < 4 or (dz == 4 and step == 0)
            a = step if near < 4 else 1 - step
            if dz == 4:
                a = step
            i = HELD[near, k]
            if k == 0 and step == 0:
                if dz < 4:
                    done(rb.at[near], rb_r.at[near])
                    if near != 5:
                        rb_push(near, plus)
            done(bk.at[i, a], z_r.at[i, a])
            if dz == 4:
                return
            to = toward(near, plus)[0]
            if k in BRINGS[to] and (to != 4 or step == 0):
                z_push(near, k, plus, a)

    def rb_push(dz, plus):
        if plus:
            to, dev, i = dz + 1, at_z(1), 0
        else:
            to, dev, i = (dz + NZ - 1) % NZ, at_z(NZ - 1), 1
        push(rb.at[dz], rb.at[to], rb_s, rb_r.at[to], dev)

    @jax.named_scope("slots_of")
    def slots_of(dz):
        pos = POS[dz]
        e16 = lax.broadcasted_iota(I32, (16, TOK), 0)
        target = ((e16 // 4 - y) & 3) * NC + (((e16 // 2) - c) & 1)
        base = (target * SLOT + (e16 & 1) * CAP).astype(F32)
        block = rb[dz]
        chosen = block[0:2].astype(I32) - z * 16
        e0 = (e16 == chosen[0:1]).astype(F32)
        e1 = (e16 == chosen[1:2]).astype(F32)
        both = jnp.concatenate([e0, e1], axis=0).astype(BF16)
        before = jnp.dot(both, upper[...], preferred_element_type=F32)
        before0 = before[0:16]
        before1 = before[16:32] + jnp.sum(e0, axis=1, keepdims=True)
        s0 = jnp.sum(e0 * (base + before0 + 1.0), axis=0, keepdims=True) - 1.0
        s1 = jnp.sum(e1 * (base + before1 + 1.0), axis=0, keepdims=True) - 1.0
        slots = jnp.concatenate([s0, s1], axis=0).astype(I32)
        sl[pos, 0:2] = slots
        row = lax.broadcasted_iota(I32, (ROWS, TOK), 0)
        p0 = row == slots[0:1]
        p1 = row == slots[1:2]
        pk[pos] = (p0 | p1).astype(F32).astype(BF16)
        weight = jnp.sum(
            jnp.where(p0, block[2:3], 0.0) + jnp.where(p1, block[3:4], 0.0),
            axis=1, keepdims=True,
        )
        wt[pos] = jnp.broadcast_to(weight, (ROWS, FS))

    @jax.named_scope("build")
    def build(dz, k):
        pos, b = POS[dz], BUILT[dz, k]
        src, stage, land = bk.at[HELD[dz, k]], sx.at[b], rq.at[k, pos]
        pick = pk[pos]
        w = jnp.concatenate([wt[pos], wt[pos]], axis=1)
        t = jnp.dot(pick, src[0], preferred_element_type=F32)
        s = jnp.dot(pick, src[1], preferred_element_type=F32) * w
        t = t.reshape(PLANE, 3, 8, Q).astype(BF16)
        s = s.reshape(PLANE, 3, 8, Q).astype(BF16)
        stage[:, 0:3] = t
        stage[:, 3:6] = s
        land[0, 0:3] = t[0]
        land[0, 3:6] = s[0]
        for j in range(1, PLANE):
            push(stage.at[j], land.at[j], ip_s, ip_r.at[b], at_plane(j, 1))

    def landed(dz, k):
        done(rq.at[k, POS[dz], pl.ds(1, PLANE - 1)], ip_r.at[BUILT[dz, k]])

    @jax.named_scope("x_push")
    def x_push(dz):
        pos = POS[dz]
        landed(dz, 0)
        count["x"] += (1 not in BRINGS[dz]) + (2 not in BRINGS[dz])
        if 1 not in BRINGS[dz]:
            push(rq.at[0, pos], rq.at[1, pos], x_s, x_r.at[0, pos], at_x(1))
        if 2 not in BRINGS[dz]:
            push(rq.at[0, pos], rq.at[2, pos], x_s, x_r.at[1, pos], at_x(NX - 1))

    low, high = pl.ds(0, PLANE // 2), pl.ds(PLANE // 2, PLANE // 2)

    @jax.named_scope("x_pass")
    def x_pass(dz):
        pos = POS[dz]
        done(rq.at[1, pos], x_r.at[0, pos])
        push(rq.at[1, pos, low], rq.at[3, pos, low], xf_s, xf_r.at[0], at_x(1))
        done(rq.at[2, pos], x_r.at[1, pos])
        push(
            rq.at[2, pos, high], rq.at[3, pos, high], xf_s, xf_r.at[1],
            at_x(NX - 1),
        )

    @jax.named_scope("compute_wait")
    def compute_wait(*blocks):
        for dz in blocks:
            pos, own = POS[dz], BRINGS[dz]
            for k in own:
                if k:
                    landed(dz, k)
            if 3 not in own:
                done(rq.at[3, pos, low], xf_r.at[0])
                done(rq.at[3, pos, high], xf_r.at[1])
            else:
                for k in (1, 2):
                    if k not in own:
                        done(rq.at[k, pos], x_r.at[k - 1, pos])

    @jax.named_scope("compute")
    def compute(*blocks):
        p, n = POS[blocks[0]], len(blocks)
        m = n * ROWS
        rows = pl.ds(p * ROWS, m)
        pre = jnp.zeros((m, 512), F32)
        hg = jnp.zeros((m, 256), F32)
        for k in range(4):
            src = rq.at[k]
            t = src[p:p + n, :, 0:3].astype(F32).reshape(m, Q).astype(BF16)
            s = src[p:p + n, :, 3:6].astype(F32).reshape(m, Q).astype(BF16)
            ts[k, 0, rows] = t
            ts[k, 1, rows] = s
            pre = pre + jnp.dot(t, wgu[quarter(k)], preferred_element_type=F32)
            hg = hg + lax.dot_general(
                s, wds[quarter(k)], CONTRACT_MINOR, preferred_element_type=F32
            )
        first = first_of(n, FS)
        g = jnp.where(first, pre[:, 0:128], pre[:, 128:256]).astype(BF16).astype(F32)
        u = jnp.where(first, pre[:, 256:384], pre[:, 384:512]).astype(BF16).astype(F32)
        dh = jnp.where(first, hg[:, 0:128], hg[:, 128:256])
        sg = jax.nn.sigmoid(g)
        act = g * sg
        hidden = act * u
        product = jnp.sum(dh * hidden, axis=1, keepdims=True)
        for i in range(n):
            spread = jnp.broadcast_to(product[i * ROWS:(i + 1) * ROWS], (ROWS, FS))
            placed = jnp.where(lane_of_slot(p + i), spread.reshape(PLANE, SLOT, FS), 0.0)
            pr[(p + i) // 4] += jnp.sum(placed, axis=1)
        gg = dh * u * sg * (1.0 + g * (1.0 - sg))
        ug = dh * act
        gx[0, rows, 0:FS] = gg.astype(BF16)
        gx[0, rows, FS:2 * FS] = ug.astype(BF16)
        for i, v in enumerate((gg, ug, hidden)):
            lo = jnp.where(first, v, 0.0).astype(BF16)
            hi = jnp.where(first, 0.0, v).astype(BF16)
            if i < 2:
                gu2[rows, 256 * i:256 * i + 128] = lo
                gu2[rows, 256 * i + 128:256 * i + 256] = hi
            else:
                h2[rows, 0:128] = lo
                h2[rows, 128:256] = hi

    @jax.named_scope("weight_grads")
    def weight_grads(k):
        at = pl.ds(pl.multiple_of(quarter(k) * Q, Q), Q)
        o = lax.dot_general(ts[k, 0], gu2[...], CONTRACT_MAJOR, preferred_element_type=F32)
        for i in range(2):
            dg[i, at, :] = o[:, i * FS:(i + 1) * FS]
            du[i, at, :] = o[:, 256 + i * FS:256 + (i + 1) * FS]
        o = lax.dot_general(h2[...], ts[k, 1], CONTRACT_MAJOR, preferred_element_type=F32)
        for i in range(2):
            dd[i, :, at] = o[i * FS:(i + 1) * FS]

    def rows_of(dz, lo=0, n=ROWS):
        return pl.ds(POS[dz] * ROWS + lo, n)

    def g_push(dz):
        r = rows_of(dz)
        push(gx.at[0, r], gx.at[1, r], g_s, g_r.at[0, dz], at_x(1))
        push(gx.at[0, r], gx.at[2, r], g_s, g_r.at[1, dz], at_x(NX - 1))

    @jax.named_scope("g_pass")
    def g_pass(dz):
        lo, hi = rows_of(dz, 0, 96), rows_of(dz, 96, 96)
        done(gx.at[1, rows_of(dz)], g_r.at[0, dz])
        push(gx.at[1, lo], gx.at[3, lo], gf_s, gf_r.at[0, dz], at_x(1))
        done(gx.at[2, rows_of(dz)], g_r.at[1, dz])
        push(gx.at[2, hi], gx.at[3, hi], gf_s, gf_r.at[1, dz], at_x(NX - 1))

    @jax.named_scope("ig_wait")
    def ig_wait(dz):
        done(gx.at[3, rows_of(dz, 0, 96)], gf_r.at[0, dz])
        done(gx.at[3, rows_of(dz, 96, 96)], gf_r.at[1, dz])

    @jax.named_scope("input_grad")
    def input_grad(dz):
        pos = POS[dz]
        first = first_of(1, FS)
        total = jnp.zeros((ROWS, Q), F32)
        for slot, w in ((0, None), (1, 0), (2, 2), (3, 1)):
            pair = gx[slot, rows_of(dz)].astype(F32)
            gg, ug = pair[:, 0:FS], pair[:, FS:2 * FS]
            lhs = jnp.concatenate(
                [
                    jnp.where(first, gg, 0.0).astype(BF16),
                    jnp.where(first, 0.0, gg).astype(BF16),
                    jnp.where(first, ug, 0.0).astype(BF16),
                    jnp.where(first, 0.0, ug).astype(BF16),
                ],
                axis=1,
            )
            rhs = wgu[x] if w is None else wq[w]
            total = total + lax.dot_general(lhs, rhs, CONTRACT_MINOR, preferred_element_type=F32)
        igs[pos] = total
        igr[pos, 0:SLOT] = total[0:SLOT]
        for j in range(1, PLANE):
            at = pl.ds(j * SLOT, SLOT)
            push(
                igs.at[pos, at], igr.at[pos, at], ig_s, ig_r.at[pos], at_plane(j, -1),
            )

    @jax.named_scope("dense")
    def dense(dz):
        pos = POS[dz]
        with jax.named_scope("dense_wait"):
            done(igr.at[pos, pl.ds(SLOT, ROWS - SLOT)], ig_r.at[pos])
        pick = pk[pos]
        v = igr[pos]
        hi = v.astype(BF16)
        rest = v - hi.astype(F32)
        mid = rest.astype(BF16)
        low = (rest - mid.astype(F32)).astype(BF16)
        total = lax.dot_general(pick, hi, CONTRACT_MAJOR, preferred_element_type=F32)
        total = total + (
            lax.dot_general(pick, mid, CONTRACT_MAJOR, preferred_element_type=F32)
            + lax.dot_general(pick, low, CONTRACT_MAJOR, preferred_element_type=F32)
        )
        db[dz] = total

    @jax.named_scope("pair_products")
    def pair_products(dz):
        pos = POS[dz]
        row = lax.broadcasted_iota(I32, (ROWS, TOK), 0)
        slots = sl[pos, 0:2]
        spread = jnp.broadcast_to(prr[:, pos // 4][:, None, :], (PLANE, SLOT, FS))
        col = jnp.sum(
            jnp.where(lane_of_slot(pos), spread, 0.0).reshape(ROWS, FS), axis=1, keepdims=True
        )
        r0 = jnp.sum(jnp.where(row == slots[0:1], col, 0.0), axis=0, keepdims=True)
        r1 = jnp.sum(jnp.where(row == slots[1:2], col, 0.0), axis=0, keepdims=True)
        pb[dz] = jnp.concatenate([r0, r1, jnp.zeros((6, Q), F32)], axis=0)
        if dz:
            push(pb.at[dz], pe.at[dz], pz_s, pz_r, at_z(NZ - dz))

    def part(i):
        return pl.ds(PART * i, PART)

    @jax.named_scope("chain")
    def chain(dz, i):
        if dz < 4 or (dz == 4 and i < 2):
            land, at, dev = rm.at[dz - 1, part(i)], dz - 1, at_z(NZ - 1)
            if dz < 3 or (dz == 3 and i < 2):
                done(rm.at[dz, part(i)], c_r.at[i, dz])
                db[dz, part(i)] += rm[dz, part(i)]
        else:
            land, at, dev = rp.at[dz - 4, part(i)], dz, at_z(1)
            if dz > 5 or (dz == 5 and i >= 2):
                done(rp.at[dz - 5, part(i)], c_r.at[i, dz - 1])
                db[dz, part(i)] += rp[dz - 5, part(i)]
        push(db.at[dz, part(i)], land, c_s, c_r.at[i, at], dev)

    def products():
        with jax.named_scope("products"):
            done(prx, p_r)
            total = pr[...] + prx[0] + prx[1] + prx[2]
            for j in range(PLANE):
                prs[j] = total[:, j]
            prr[0] = total[:, 0]
            for j in range(1, PLANE):
                push(prs.at[j], prr.at[j], pp_s, pp_r, at_plane(j, -1))

    def put(src, dst, sem):
        pltpu.make_async_copy(src, dst, sem).start()

    def early(dz):
        for i in (0, 1):
            chain(dz, 2 + i if dz < 4 else i)

    def later(dz):
        for i in (0, 1):
            chain(dz, i if dz < 4 else 2 + i)

    def grad(dz):
        ig_wait(dz)
        input_grad(dz)

    rb_push(0, True)
    rb_push(0, False)
    z_own(0)
    slots_of(0)
    done(bk.at[pl.ds(0, 2)], in_s.at[3])
    done(wv, in_s.at[4])
    for k in BRINGS[0]:
        build(0, k)
    with jax.named_scope("weights"):
        for q in range(4):
            for w in range(2):
                for i in range(2):
                    lane = 256 * w + FS * i
                    wgu[q, :, lane:lane + FS] = wv[w, i, q * Q:(q + 1) * Q, :]
        for s in range(1, NX):
            push(wgu.at[(x + s) % NX], wq.at[s - 1], w_s, w_r, at_x(s))
        done(wds, in_s.at[5])

    def make(blocks, k):
        for dz in blocks:
            if k == 0:
                slots_of(dz)
            build(dz, k)

    z_take(1, 0, 0)
    z_take(1, 0, 1)
    make((1, 7), 0)
    x_push(0)
    z_take(2, 0, 0)
    z_take(2, 0, 1)
    make((2, 6), 0)
    x_push(1)
    x_push(7)
    z_take(3, 0, 0)
    z_own(3)
    x_push(2)
    z_take(3, 0, 1)
    make((3, 5), 0)
    x_push(6)
    z_take(1, 3, 0)
    with jax.named_scope("z_take"):
        done(rb.at[4], rb_r.at[4])
        z_take(4, 0, 0)
        z_take(4, 0, 1)
    make((4,), 0)
    z_take(1, 3, 1)
    make((1, 7), 3)
    compute_wait(0)
    compute(0)
    x_push(3)
    x_push(5)
    x_push(4)
    z_take(2, 3, 0)
    z_take(2, 3, 1)
    make((2, 6), 3)
    z_take(3, 3, 0)
    for step in range(2):
        z_push(0, 2, True, step)
        z_push(0, 1, False, 1 - step)
    z_take(3, 3, 1)
    make((3, 5), 3)
    compute_wait(2, 6)
    compute(2, 6)
    g_push(2)
    x_pass(4)
    g_push(6)
    compute_wait(3, 5)
    compute(3, 5)
    with jax.named_scope("z_extra"):
        done(bk.at[HELD[1, 2], 0], z_r.at[HELD[1, 2], 0])
        done(bk.at[HELD[1, 2], 1], z_r.at[HELD[1, 2], 1])
        done(bk.at[HELD[7, 1], 0], z_r.at[HELD[7, 1], 0])
        done(bk.at[HELD[7, 1], 1], z_r.at[HELD[7, 1], 1])
    build(1, 2)
    build(7, 1)
    g_pass(2)
    compute_wait(4)
    compute(4)
    g_push(4)
    g_pass(6)
    g_push(3)
    with jax.named_scope("wq_wait"):
        done(wq, w_r)
    grad(2)
    g_pass(4)
    g_push(5)
    grad(6)
    compute_wait(1, 7)
    compute(1, 7)
    g_pass(3)
    g_push(1)
    grad(4)

    for s in range(1, NX):
        push(pr, prx.at[s - 1], p_s, p_r, at_x(s))
    g_pass(5)
    g_push(7)
    dense(2)
    dense(6)
    grad(3)
    products()
    g_pass(1)
    g_push(0)
    dense(4)
    for i in range(4):
        chain(4, i)
    grad(5)
    dense(3)
    early(3)
    g_pass(7)
    later(3)
    grad(1)
    dense(5)
    early(5)
    later(5)
    g_pass(0)
    early(2)
    grad(7)
    later(2)
    early(6)
    dense(1)
    early(1)
    later(6)
    grad(0)
    later(1)
    dense(7)
    early(7)
    later(7)
    with jax.named_scope("products_wait"):
        done(prr.at[pl.ds(1, PLANE - 1)], pp_r)
    for dz in (4, 3, 5, 2, 6, 1, 7, 0):
        pair_products(dz)
    dense(0)
    with jax.named_scope("early_final"):
        for i in (0, 1):
            done(rm.at[0, part(2 + i)], c_r.at[2 + i, 0])
            db[0, part(2 + i)] += rm[0, part(2 + i)]
            done(rp.at[3, part(i)], c_r.at[i, 7])
            db[0, part(i)] += rp[3, part(i)]

    mine = pl.ds(pl.multiple_of(x * Q, Q), Q)
    with jax.named_scope("final"):
        for i in (0, 2, 1, 3):
            got, sem = (rm.at[0], c_r.at[i, 0]) if i < 2 else (rp.at[3], c_r.at[i, 7])
            done(got.at[part(i)], sem)
            tq[part(i)] = (db[0, part(i)] + got[part(i)]).astype(BF16)
            src, dst = tq.at[part(i)], tg_out.at[part(i), mine]
            for k in range(1, NX):
                push(src, dst, t_s, t_r, at_x(k))
        put(tq, tg_out.at[:, mine], out_s.at[0])
    for k in range(4):
        weight_grads(k)
        at = pl.ds(pl.multiple_of(quarter(k) * Q, Q), Q)
        put(dg.at[:, at], dg_out.at[:, at], out_s.at[1])
        put(du.at[:, at], du_out.at[:, at], out_s.at[2])
        put(dd.at[:, :, at], dd_out.at[:, :, at], out_s.at[3])
    done(pe.at[pl.ds(1, NZ - 1)], pz_r)
    total = pb[0]
    for dz in range(1, NZ):
        total = total + pe[dz]
    gg[...] = total[0:2] / gw[...]
    put(gg, gg_out, out_s.at[4])
    with jax.named_scope("gather"):
        done(gx.at[0, pl.ds(0, 3 * TOK)], t_r)
    with jax.named_scope("drain"):
        done(bk.at[pl.ds(0, count["z"] // 2)], z_s)
        done(rb.at[pl.ds(0, 7)], rb_s)
        done(sx.at[:, pl.ds(1, PLANE - 1)], ip_s)
        done(rq.at[pl.ds(0, 2), pl.ds(0, count["x"] // 2)], x_s)
        done(rq.at[0, 0], xf_s)
        done(wq, w_s)
        done(gx.at[pl.ds(0, 2)], g_s)
        done(gx.at[0], gf_s)
        done(prx, p_s)
        done(prs.at[pl.ds(1, PLANE - 1)], pp_s)
        done(pb.at[pl.ds(0, NZ - 1)], pz_s)
        done(igs.at[:, pl.ds(SLOT, ROWS - SLOT)], ig_s)
        done(db.at[pl.ds(0, 7)], c_s)
        done(gx.at[0, pl.ds(0, 3 * TOK)], t_s)
        done(tq, out_s.at[0])
        done(dg, out_s.at[1])
        done(du, out_s.at[2])
        done(dd, out_s.at[3])
        done(gg, out_s.at[4])


def carry(tg, gg, dg, du, dd, tg_out, gg_out, dg_out, du_out, dd_out, tg_v, gg_v, w_v, d_v, in_s, out_s):
    pairs = [(tg, tg_v, tg_out), (gg, gg_v, gg_out)]
    for i, (a, b) in enumerate(((dg, dg_out), (du, du_out), (dd, dd_out))):
        for k in range(2):
            pairs.append((a.at[k], w_v.at[2 * i + k] if i < 2 else d_v.at[k], b.at[k]))
    views = []
    for i, (a, v, b) in enumerate(pairs):
        views.append((pltpu.make_async_copy(a, v, in_s.at[i]), pltpu.make_async_copy(v, b, out_s.at[i])))
    for load, _ in views:
        load.start()
    for load, store in views:
        load.wait()
        store.start()
    for _, store in views:
        store.wait()


def shards(tokens, cotangent, routing, gate_weights, gate_proj, up_proj, down_proj):
    hbm = pl.BlockSpec(memory_space=pl.ANY)
    dma = pltpu.SemaphoreType.DMA
    scratch = [
        pltpu.VMEM((2, TOK), I32),
        pltpu.VMEM((2, TOK), F32),
        pltpu.VMEM((2, TOK), F32),
        pltpu.VMEM((len(HELD), 2, TOK, Q), BF16),
        pltpu.VMEM((NZ, 8, TOK), F32),
        pltpu.VMEM((len(BUILT), PLANE, 6, 8, Q), BF16),
        pltpu.VMEM((4, NZ, PLANE, 6, 8, Q), BF16),
        pltpu.VMEM((2, 2, D, FS), BF16),
        pltpu.VMEM((4, Q, 512), BF16),
        pltpu.VMEM((4, 256, Q), BF16),
        pltpu.VMEM((3, Q, 512), BF16),
        pltpu.VMEM((NZ, 8, TOK), I32),
        pltpu.VMEM((TOK, TOK), BF16),
        pltpu.VMEM((NZ, ROWS, TOK), BF16),
        pltpu.VMEM((NZ, ROWS, FS), F32),
        pltpu.VMEM((4, 2, ALL, Q), BF16),
        pltpu.VMEM((ALL, 512), BF16),
        pltpu.VMEM((ALL, 256), BF16),
        pltpu.VMEM((4, ALL, 256), BF16),
        pltpu.VMEM((2, PLANE, FS), F32),
        pltpu.VMEM((3, 2, PLANE, FS), F32),
        pltpu.VMEM((PLANE, 2, FS), F32),
        pltpu.VMEM((PLANE, 2, FS), F32),
        pltpu.VMEM((NZ, 8, Q), F32),
        pltpu.VMEM((NZ, 8, Q), F32),
        pltpu.VMEM((NZ, ROWS, Q), F32),
        pltpu.VMEM((NZ, ROWS, Q), F32),
        pltpu.VMEM((NZ, TOK, Q), F32),
        pltpu.VMEM((4, TOK, Q), F32),
        pltpu.VMEM((4, TOK, Q), F32),
        pltpu.VMEM((TOK, Q), BF16),
        pltpu.VMEM((2, D, FS), F32),
        pltpu.VMEM((2, D, FS), F32),
        pltpu.VMEM((2, FS, D), F32),
        dma((6,)), dma, dma((len(HELD), 2)), dma, dma((8,)),
        dma, dma((len(BUILT),)),
        dma, dma((2, 8)), dma, dma((2,)),
        dma, dma, dma, dma((2, 8)), dma, dma((2, 8)),
        dma, dma, dma, dma, dma, dma, dma, dma((8,)),
        dma, dma((4, 8)), dma, dma, dma((5,)),
    ]
    tg, gg, dg, du, dd = pl.pallas_call(
        kernel,
        out_shape=(
            jax.ShapeDtypeStruct((TOK, D), BF16),
            jax.ShapeDtypeStruct((2, TOK), F32),
            jax.ShapeDtypeStruct((2, D, FS), F32),
            jax.ShapeDtypeStruct((2, D, FS), F32),
            jax.ShapeDtypeStruct((2, FS, D), F32),
        ),
        in_specs=[hbm] * 7,
        out_specs=(hbm,) * 5,
        scratch_shapes=scratch,
        compiler_params=pltpu.CompilerParams(
            collective_id=0, has_side_effects=True, vmem_limit_bytes=63 * 1024 * 1024
        ),
    )(tokens, cotangent, routing.T, gate_weights.T, gate_proj, up_proj, down_proj)
    wide = jax.ShapeDtypeStruct((2, D, FS), F32)
    tg, gg, dg, du, dd = pl.pallas_call(
        carry,
        out_shape=(
            jax.ShapeDtypeStruct((TOK, D), BF16),
            jax.ShapeDtypeStruct((2, TOK), F32),
            wide, wide,
            jax.ShapeDtypeStruct((2, FS, D), F32),
        ),
        in_specs=[hbm] * 5,
        out_specs=(hbm,) * 5,
        scratch_shapes=[
            pltpu.VMEM((TOK, D), BF16),
            pltpu.VMEM((2, TOK), F32),
            pltpu.VMEM((4, D, FS), F32),
            pltpu.VMEM((2, FS, D), F32),
            dma((8,)),
            dma((8,)),
        ],
        compiler_params=pltpu.CompilerParams(vmem_limit_bytes=63 * 1024 * 1024),
    )(tg, gg, dg, du, dd)
    return tg, gg.T, dg, du, dd


def solution(mesh):
    in_specs = (
        P("ep", None),
        P("ep", None),
        P("ep", None),
        P("ep", None),
        P("ep", None, "tp"),
        P("ep", None, "tp"),
        P("ep", "tp", None),
    )
    out_specs = (
        P("ep", None),
        P("ep", None),
        P("ep", None, "tp"),
        P("ep", None, "tp"),
        P("ep", "tp", None),
    )
    return jax.shard_map(shards, mesh=mesh, in_specs=in_specs, out_specs=out_specs, check_vma=False)
```

```python
import jax
import jax.numpy as jnp
from jax import lax
from jax.experimental import pallas as pl
from jax.experimental.pallas import tpu as pltpu
from jax.sharding import PartitionSpec as P

F32 = jnp.float32
BF16 = jnp.bfloat16
I32 = jnp.int32
MESH = pl.DeviceIdType.MESH

NZ, NY, NC, NX = 8, 4, 2, 4
PLANE = NY * NC
TOK = 256
D = 1024
Q = 256
FS = 128
CAP = 12
SLOT = 2 * CAP
ROWS = PLANE * SLOT
ALL = NZ * ROWS
POS = {0: 0, 1: 1, 7: 2, 2: 3, 6: 4, 3: 5, 5: 6, 4: 7}
BRINGS = {
    0: (0, 3), 1: (0, 3, 2), 2: (0, 3), 3: (0, 3), 4: (0,), 5: (0, 3), 6: (0, 3), 7: (0, 3, 1),
}
HELD = [(0, k) for k in range(4)]
HELD += [(dz, k) for dz in (1, 2, 3, 5, 6, 7, 4) for k in BRINGS[dz]]
HELD = {key: i for i, key in enumerate(HELD)}
BUILT = {key: i for i, key in enumerate((dz, k) for dz in range(NZ) for k in BRINGS[dz])}
PART = TOK // 4
CONTRACT_MINOR = (((1,), (1,)), ((), ()))
CONTRACT_MAJOR = (((0,), (0,)), ((), ()))


def kernel(
    tok, cot, rt_in, gw_in, wg, wu, wd,
    tg_out, gg_out, dg_out, du_out, dd_out,
    rt, gw, gg, bk, rb, sx, rq, wv, wgu, wds, wq, sl, upper, pk, wt, ts, gu2, h2,
    gx, pr, prx, prs, prr, pb, pe, igs, igr, db, rm, rp, tq, dg, du, dd,
    in_s, z_s, z_r, rb_s, rb_r, ip_s, ip_r, x_s, x_r, xf_s, xf_r, w_s, w_r, g_s, g_r, gf_s, gf_r,
    p_s, p_r, pp_s, pp_r, pz_s, pz_r, ig_s, ig_r, c_s, c_r, t_s, t_r, out_s,
):
    e = lax.axis_index("ep")
    x = lax.axis_index("tp")
    z = e // PLANE
    y = (e % PLANE) // NC
    c = e % NC

    def at_z(step):
        return (((z + step) % NZ) * PLANE + y * NC + c, x)

    def at_plane(j, sign):
        dy, dc = j // NC, j % NC
        return (z * PLANE + ((y + sign * dy + NY) % NY) * NC + (c + dc) % NC, x)

    def at_x(step):
        return (e, (x + step) % NX)

    def remote(src, dst, ssem, rsem, dev):
        return pltpu.make_async_remote_copy(
            src_ref=src, dst_ref=dst, send_sem=ssem, recv_sem=rsem,
            device_id=dev, device_id_type=MESH,
        )

    def done(ref, sem):
        pltpu.make_async_copy(ref, ref, sem).wait()

    def push(src, dst, ssem, rsem, dev):
        remote(src, dst, ssem, rsem, dev).start()

    def quarter(k):
        who = (x + (0, NX - 1, 1, 2)[k]) % NX
        return 2 * (who % 2) + who // 2

    with jax.named_scope("prologue"):
        barrier = pltpu.get_barrier_semaphore()
        partners = [at_z(k) for k in range(1, NZ)]
        partners += [at_plane(j, 1) for j in range(1, PLANE)]
        partners += [at_x(s) for s in range(1, NX)]
        for dev in partners:
            pl.semaphore_signal(barrier, inc=1, device_id=dev, device_id_type=MESH)

        loads = [
            pltpu.make_async_copy(rt_in, rt, in_s.at[0]),
            pltpu.make_async_copy(gw_in, gw, in_s.at[1]),
        ]
        for k in (0, 3, 1, 2):
            cols = pl.ds(pl.multiple_of(quarter(k) * Q, Q), Q)
            dst = bk.at[HELD[0, k]]
            loads.append(pltpu.make_async_copy(tok.at[:, cols], dst.at[0], in_s.at[2 if k in (0, 3) else 3]))
            loads.append(pltpu.make_async_copy(cot.at[:, cols], dst.at[1], in_s.at[2 if k in (0, 3) else 3]))
        for i, w in enumerate((wg, wu)):
            loads.append(pltpu.make_async_copy(w, wv.at[i], in_s.at[4]))
        for q in range(4):
            for i in range(2):
                loads.append(
                    pltpu.make_async_copy(
                        wd.at[i, :, pl.ds(q * Q, Q)], wds.at[q, pl.ds(i * FS, FS)], in_s.at[5]
                    )
                )
        for load in loads:
            load.start()
        upper[...] = (
            lax.broadcasted_iota(I32, (TOK, TOK), 0) < lax.broadcasted_iota(I32, (TOK, TOK), 1)
        ).astype(F32).astype(BF16)
        pr[...] = jnp.zeros_like(pr)
        loads[0].wait()
        loads[1].wait()
        done(bk.at[pl.ds(0, 2)], in_s.at[2])
        rb[0] = jnp.concatenate(
            [rt[...].astype(F32), gw[...], jnp.zeros((4, TOK), F32)], axis=0
        )
    with jax.named_scope("barrier"):
        pl.semaphore_wait(barrier, len(partners))

    def first_of(n, lanes):
        i = lax.broadcasted_iota(I32, (n * PLANE, SLOT, lanes), 1)
        return (i < CAP).reshape(n * ROWS, lanes)

    def lane_of_slot(pos):
        i = lax.broadcasted_iota(I32, (PLANE, SLOT, FS), 1)
        l = lax.broadcasted_iota(I32, (PLANE, SLOT, FS), 2)
        return i + 32 * (pos % 4) == l

    def toward(dz, plus):
        return (dz + 1, at_z(1)) if plus else ((dz + NZ - 1) % NZ, at_z(NZ - 1))

    count = {"z": 0, "x": 0}

    def z_push(dz, k, plus, a):
        to, dev = toward(dz, plus)
        i = HELD[to, k]
        count["z"] += 1
        push(bk.at[HELD[dz, k], a], bk.at[i, a], z_s, z_r.at[i, a], dev)

    def z_own(k):
        for step in range(2):
            z_push(0, k, True, step)
            z_push(0, k, False, 1 - step)

    @jax.named_scope("z_take")
    def z_take(dz, k, step):
        for near in (dz, NZ - dz):
            plus = near < 4 or (dz == 4 and step == 0)
            a = step if near < 4 else 1 - step
            if dz == 4:
                a = step
            i = HELD[near, k]
            if k == 0 and step == 0:
                if dz < 4:
                    done(rb.at[near], rb_r.at[near])
                    if near != 5:
                        rb_push(near, plus)
            done(bk.at[i, a], z_r.at[i, a])
            if dz == 4:
                return
            to = toward(near, plus)[0]
            if k in BRINGS[to] and (to != 4 or step == 0):
                z_push(near, k, plus, a)

    def rb_push(dz, plus):
        if plus:
            to, dev, i = dz + 1, at_z(1), 0
        else:
            to, dev, i = (dz + NZ - 1) % NZ, at_z(NZ - 1), 1
        push(rb.at[dz], rb.at[to], rb_s, rb_r.at[to], dev)

    @jax.named_scope("slots_of")
    def slots_of(dz):
        pos = POS[dz]
        e16 = lax.broadcasted_iota(I32, (16, TOK), 0)
        target = ((e16 // 4 - y) & 3) * NC + (((e16 // 2) - c) & 1)
        base = (target * SLOT + (e16 & 1) * CAP).astype(F32)
        block = rb[dz]
        chosen = block[0:2].astype(I32) - z * 16
        e0 = (e16 == chosen[0:1]).astype(F32)
        e1 = (e16 == chosen[1:2]).astype(F32)
        both = jnp.concatenate([e0, e1], axis=0).astype(BF16)
        before = jnp.dot(both, upper[...], preferred_element_type=F32)
        before0 = before[0:16]
        before1 = before[16:32] + jnp.sum(e0, axis=1, keepdims=True)
        s0 = jnp.sum(e0 * (base + before0 + 1.0), axis=0, keepdims=True) - 1.0
        s1 = jnp.sum(e1 * (base + before1 + 1.0), axis=0, keepdims=True) - 1.0
        slots = jnp.concatenate([s0, s1], axis=0).astype(I32)
        sl[pos, 0:2] = slots
        row = lax.broadcasted_iota(I32, (ROWS, TOK), 0)
        p0 = row == slots[0:1]
        p1 = row == slots[1:2]
        pk[pos] = (p0 | p1).astype(F32).astype(BF16)
        weight = jnp.sum(
            jnp.where(p0, block[2:3], 0.0) + jnp.where(p1, block[3:4], 0.0),
            axis=1, keepdims=True,
        )
        wt[pos] = jnp.broadcast_to(weight, (ROWS, FS))

    @jax.named_scope("build")
    def build(dz, k):
        pos, b = POS[dz], BUILT[dz, k]
        src, stage, land = bk.at[HELD[dz, k]], sx.at[b], rq.at[k, pos]
        pick = pk[pos]
        w = jnp.concatenate([wt[pos], wt[pos]], axis=1)
        t = jnp.dot(pick, src[0], preferred_element_type=F32)
        s = jnp.dot(pick, src[1], preferred_element_type=F32) * w
        t = t.reshape(PLANE, 3, 8, Q).astype(BF16)
        s = s.reshape(PLANE, 3, 8, Q).astype(BF16)
        stage[:, 0:3] = t
        stage[:, 3:6] = s
        land[0, 0:3] = t[0]
        land[0, 3:6] = s[0]
        for j in range(1, PLANE):
            push(stage.at[j], land.at[j], ip_s, ip_r.at[b], at_plane(j, 1))

    def landed(dz, k):
        done(rq.at[k, POS[dz], pl.ds(1, PLANE - 1)], ip_r.at[BUILT[dz, k]])

    @jax.named_scope("x_push")
    def x_push(dz):
        pos = POS[dz]
        landed(dz, 0)
        count["x"] += (1 not in BRINGS[dz]) + (2 not in BRINGS[dz])
        if 1 not in BRINGS[dz]:
            push(rq.at[0, pos], rq.at[1, pos], x_s, x_r.at[0, pos], at_x(1))
        if 2 not in BRINGS[dz]:
            push(rq.at[0, pos], rq.at[2, pos], x_s, x_r.at[1, pos], at_x(NX - 1))

    low, high = pl.ds(0, PLANE // 2), pl.ds(PLANE // 2, PLANE // 2)

    @jax.named_scope("x_pass")
    def x_pass(dz):
        pos = POS[dz]
        done(rq.at[1, pos], x_r.at[0, pos])
        push(rq.at[1, pos, low], rq.at[3, pos, low], xf_s, xf_r.at[0], at_x(1))
        done(rq.at[2, pos], x_r.at[1, pos])
        push(
            rq.at[2, pos, high], rq.at[3, pos, high], xf_s, xf_r.at[1],
            at_x(NX - 1),
        )

    @jax.named_scope("compute_wait")
    def compute_wait(*blocks):
        for dz in blocks:
            pos, own = POS[dz], BRINGS[dz]
            for k in own:
                if k:
                    landed(dz, k)
            if 3 not in own:
                done(rq.at[3, pos, low], xf_r.at[0])
                done(rq.at[3, pos, high], xf_r.at[1])
            else:
                for k in (1, 2):
                    if k not in own:
                        done(rq.at[k, pos], x_r.at[k - 1, pos])

    @jax.named_scope("compute")
    def compute(*blocks):
        p, n = POS[blocks[0]], len(blocks)
        m = n * ROWS
        rows = pl.ds(p * ROWS, m)
        pre = jnp.zeros((m, 512), F32)
        hg = jnp.zeros((m, 256), F32)
        for k in range(4):
            src = rq.at[k]
            t = src[p:p + n, :, 0:3].astype(F32).reshape(m, Q).astype(BF16)
            s = src[p:p + n, :, 3:6].astype(F32).reshape(m, Q).astype(BF16)
            ts[k, 0, rows] = t
            ts[k, 1, rows] = s
            pre = pre + jnp.dot(t, wgu[quarter(k)], preferred_element_type=F32)
            hg = hg + lax.dot_general(
                s, wds[quarter(k)], CONTRACT_MINOR, preferred_element_type=F32
            )
        first = first_of(n, FS)
        g = jnp.where(first, pre[:, 0:128], pre[:, 128:256]).astype(BF16).astype(F32)
        u = jnp.where(first, pre[:, 256:384], pre[:, 384:512]).astype(BF16).astype(F32)
        dh = jnp.where(first, hg[:, 0:128], hg[:, 128:256])
        sg = jax.nn.sigmoid(g)
        act = g * sg
        hidden = act * u
        product = jnp.sum(dh * hidden, axis=1, keepdims=True)
        for i in range(n):
            spread = jnp.broadcast_to(product[i * ROWS:(i + 1) * ROWS], (ROWS, FS))
            placed = jnp.where(lane_of_slot(p + i), spread.reshape(PLANE, SLOT, FS), 0.0)
            pr[(p + i) // 4] += jnp.sum(placed, axis=1)
        gg = dh * u * sg * (1.0 + g * (1.0 - sg))
        ug = dh * act
        gx[0, rows, 0:FS] = gg.astype(BF16)
        gx[0, rows, FS:2 * FS] = ug.astype(BF16)
        for i, v in enumerate((gg, ug, hidden)):
            lo = jnp.where(first, v, 0.0).astype(BF16)
            hi = jnp.where(first, 0.0, v).astype(BF16)
            if i < 2:
                gu2[rows, 256 * i:256 * i + 128] = lo
                gu2[rows, 256 * i + 128:256 * i + 256] = hi
            else:
                h2[rows, 0:128] = lo
                h2[rows, 128:256] = hi

    @jax.named_scope("weight_grads")
    def weight_grads(k):
        at = pl.ds(pl.multiple_of(quarter(k) * Q, Q), Q)
        o = lax.dot_general(ts[k, 0], gu2[...], CONTRACT_MAJOR, preferred_element_type=F32)
        for i in range(2):
            dg[i, at, :] = o[:, i * FS:(i + 1) * FS]
            du[i, at, :] = o[:, 256 + i * FS:256 + (i + 1) * FS]
        o = lax.dot_general(h2[...], ts[k, 1], CONTRACT_MAJOR, preferred_element_type=F32)
        for i in range(2):
            dd[i, :, at] = o[i * FS:(i + 1) * FS]

    def rows_of(dz, lo=0, n=ROWS):
        return pl.ds(POS[dz] * ROWS + lo, n)

    def g_push(dz):
        r = rows_of(dz)
        push(gx.at[0, r], gx.at[1, r], g_s, g_r.at[0, dz], at_x(1))
        push(gx.at[0, r], gx.at[2, r], g_s, g_r.at[1, dz], at_x(NX - 1))

    @jax.named_scope("g_pass")
    def g_pass(dz):
        lo, hi = rows_of(dz, 0, 96), rows_of(dz, 96, 96)
        done(gx.at[1, rows_of(dz)], g_r.at[0, dz])
        push(gx.at[1, lo], gx.at[3, lo], gf_s, gf_r.at[dz], at_x(1))
        done(gx.at[2, rows_of(dz)], g_r.at[1, dz])
        push(gx.at[2, hi], gx.at[3, hi], gf_s, gf_r.at[dz], at_x(NX - 1))

    @jax.named_scope("ig_wait")
    def ig_wait(dz):
        done(gx.at[3, rows_of(dz)], gf_r.at[dz])

    @jax.named_scope("input_grad")
    def input_grad(dz):
        pos = POS[dz]
        first = first_of(1, FS)
        total = jnp.zeros((ROWS, Q), F32)
        for slot, w in ((0, None), (1, 0), (2, 2), (3, 1)):
            pair = gx[slot, rows_of(dz)].astype(F32)
            gg, ug = pair[:, 0:FS], pair[:, FS:2 * FS]
            lhs = jnp.concatenate(
                [
                    jnp.where(first, gg, 0.0).astype(BF16),
                    jnp.where(first, 0.0, gg).astype(BF16),
                    jnp.where(first, ug, 0.0).astype(BF16),
                    jnp.where(first, 0.0, ug).astype(BF16),
                ],
                axis=1,
            )
            rhs = wgu[x] if w is None else wq[w]
            total = total + lax.dot_general(lhs, rhs, CONTRACT_MINOR, preferred_element_type=F32)
        igs[pos] = total
        igr[pos, 0:SLOT] = total[0:SLOT]
        for j in range(1, PLANE):
            at = pl.ds(j * SLOT, SLOT)
            push(
                igs.at[pos, at], igr.at[pos, at], ig_s, ig_r.at[pos], at_plane(j, -1),
            )

    @jax.named_scope("dense")
    def dense(dz):
        pos = POS[dz]
        with jax.named_scope("dense_wait"):
            done(igr.at[pos, pl.ds(SLOT, ROWS - SLOT)], ig_r.at[pos])
        pick = pk[pos]
        v = igr[pos]
        hi = v.astype(BF16)
        rest = v - hi.astype(F32)
        mid = rest.astype(BF16)
        low = (rest - mid.astype(F32)).astype(BF16)
        total = lax.dot_general(pick, hi, CONTRACT_MAJOR, preferred_element_type=F32)
        total = total + (
            lax.dot_general(pick, mid, CONTRACT_MAJOR, preferred_element_type=F32)
            + lax.dot_general(pick, low, CONTRACT_MAJOR, preferred_element_type=F32)
        )
        db[dz] = total

    @jax.named_scope("pair_products")
    def pair_products(dz):
        pos = POS[dz]
        row = lax.broadcasted_iota(I32, (ROWS, TOK), 0)
        slots = sl[pos, 0:2]
        spread = jnp.broadcast_to(prr[:, pos // 4][:, None, :], (PLANE, SLOT, FS))
        col = jnp.sum(
            jnp.where(lane_of_slot(pos), spread, 0.0).reshape(ROWS, FS), axis=1, keepdims=True
        )
        r0 = jnp.sum(jnp.where(row == slots[0:1], col, 0.0), axis=0, keepdims=True)
        r1 = jnp.sum(jnp.where(row == slots[1:2], col, 0.0), axis=0, keepdims=True)
        pb[dz] = jnp.concatenate([r0, r1, jnp.zeros((6, Q), F32)], axis=0)
        if dz:
            push(pb.at[dz], pe.at[dz], pz_s, pz_r, at_z(NZ - dz))

    def part(i):
        return pl.ds(PART * i, PART)

    @jax.named_scope("chain")
    def chain(dz, i):
        if dz < 4 or (dz == 4 and i < 2):
            land, at, dev = rm.at[dz - 1, part(i)], dz - 1, at_z(NZ - 1)
            if dz < 3 or (dz == 3 and i < 2):
                done(rm.at[dz, part(i)], c_r.at[i, dz])
                db[dz, part(i)] += rm[dz, part(i)]
        else:
            land, at, dev = rp.at[dz - 4, part(i)], dz, at_z(1)
            if dz > 5 or (dz == 5 and i >= 2):
                done(rp.at[dz - 5, part(i)], c_r.at[i, dz - 1])
                db[dz, part(i)] += rp[dz - 5, part(i)]
        push(db.at[dz, part(i)], land, c_s, c_r.at[i, at], dev)

    def products():
        with jax.named_scope("products"):
            done(prx, p_r)
            total = pr[...] + prx[0] + prx[1] + prx[2]
            for j in range(PLANE):
                prs[j] = total[:, j]
            prr[0] = total[:, 0]
            for j in range(1, PLANE):
                push(prs.at[j], prr.at[j], pp_s, pp_r, at_plane(j, -1))

    def put(src, dst, sem):
        pltpu.make_async_copy(src, dst, sem).start()

    def early(dz):
        for i in (0, 1):
            chain(dz, 2 + i if dz < 4 else i)

    def later(dz):
        for i in (0, 1):
            chain(dz, i if dz < 4 else 2 + i)

    def grad(dz):
        ig_wait(dz)
        input_grad(dz)

    rb_push(0, True)
    rb_push(0, False)
    z_own(0)
    slots_of(0)
    done(bk.at[pl.ds(0, 2)], in_s.at[3])
    done(wv, in_s.at[4])
    for k in BRINGS[0]:
        build(0, k)
    with jax.named_scope("weights"):
        for q in range(4):
            for w in range(2):
                for i in range(2):
                    lane = 256 * w + FS * i
                    wgu[q, :, lane:lane + FS] = wv[w, i, q * Q:(q + 1) * Q, :]
        for s in range(1, NX):
            push(wgu.at[(x + s) % NX], wq.at[s - 1], w_s, w_r, at_x(s))
        done(wds, in_s.at[5])

    def make(blocks, k):
        for dz in blocks:
            if k == 0:
                slots_of(dz)
            build(dz, k)

    z_take(1, 0, 0)
    z_take(1, 0, 1)
    make((1, 7), 0)
    x_push(0)
    z_take(2, 0, 0)
    z_take(2, 0, 1)
    make((2, 6), 0)
    x_push(1)
    x_push(7)
    z_take(3, 0, 0)
    z_own(3)
    x_push(2)
    z_take(3, 0, 1)
    make((3, 5), 0)
    x_push(6)
    z_take(1, 3, 0)
    with jax.named_scope("z_take"):
        done(rb.at[4], rb_r.at[4])
        z_take(4, 0, 0)
        z_take(4, 0, 1)
    make((4,), 0)
    z_take(1, 3, 1)
    make((1, 7), 3)
    compute_wait(0)
    compute(0)
    x_push(3)
    x_push(5)
    x_push(4)
    z_take(2, 3, 0)
    z_take(2, 3, 1)
    make((2, 6), 3)
    z_take(3, 3, 0)
    for step in range(2):
        z_push(0, 2, True, step)
        z_push(0, 1, False, 1 - step)
    z_take(3, 3, 1)
    make((3, 5), 3)
    compute_wait(2, 6)
    compute(2, 6)
    g_push(2)
    x_pass(4)
    g_push(6)
    compute_wait(3, 5)
    compute(3, 5)
    with jax.named_scope("z_extra"):
        done(bk.at[HELD[1, 2], 0], z_r.at[HELD[1, 2], 0])
        done(bk.at[HELD[1, 2], 1], z_r.at[HELD[1, 2], 1])
        done(bk.at[HELD[7, 1], 0], z_r.at[HELD[7, 1], 0])
        done(bk.at[HELD[7, 1], 1], z_r.at[HELD[7, 1], 1])
    build(1, 2)
    build(7, 1)
    g_pass(2)
    compute_wait(4)
    compute(4)
    g_push(4)
    g_pass(6)
    g_push(3)
    with jax.named_scope("wq_wait"):
        done(wq, w_r)
    grad(2)
    g_pass(4)
    g_push(5)
    grad(6)
    compute_wait(1, 7)
    compute(1, 7)
    g_pass(3)
    g_push(1)
    grad(4)

    for s in range(1, NX):
        push(pr, prx.at[s - 1], p_s, p_r, at_x(s))
    g_pass(5)
    g_push(7)
    dense(2)
    dense(6)
    grad(3)
    g_pass(1)
    g_push(0)
    dense(4)
    for i in range(4):
        chain(4, i)
    products()
    grad(5)
    dense(3)
    early(3)
    g_pass(7)
    later(3)
    dense(5)
    early(5)
    grad(1)
    early(2)
    later(5)
    g_pass(0)
    grad(7)
    later(2)
    early(6)
    dense(1)
    later(6)
    early(1)
    grad(0)
    later(1)
    dense(7)
    early(7)
    later(7)
    with jax.named_scope("products_wait"):
        done(prr.at[pl.ds(1, PLANE - 1)], pp_r)
    for dz in (4, 3, 5, 2, 6, 1, 7, 0):
        pair_products(dz)
    dense(0)
    with jax.named_scope("early_final"):
        for i in (0, 1):
            done(rm.at[0, part(2 + i)], c_r.at[2 + i, 0])
            db[0, part(2 + i)] += rm[0, part(2 + i)]
            done(rp.at[3, part(i)], c_r.at[i, 7])
            db[0, part(i)] += rp[3, part(i)]

    mine = pl.ds(pl.multiple_of(x * Q, Q), Q)
    with jax.named_scope("final"):
        for i in (0, 2, 1, 3):
            got, sem = (rm.at[0], c_r.at[i, 0]) if i < 2 else (rp.at[3], c_r.at[i, 7])
            done(got.at[part(i)], sem)
            tq[part(i)] = (db[0, part(i)] + got[part(i)]).astype(BF16)
            src, dst = tq.at[part(i)], tg_out.at[part(i), mine]
            for k in range(1, NX):
                push(src, dst, t_s, t_r, at_x(k))
        put(tq, tg_out.at[:, mine], out_s.at[0])
    for k in range(4):
        weight_grads(k)
        at = pl.ds(pl.multiple_of(quarter(k) * Q, Q), Q)
        put(dg.at[:, at], dg_out.at[:, at], out_s.at[1])
        put(du.at[:, at], du_out.at[:, at], out_s.at[2])
        put(dd.at[:, :, at], dd_out.at[:, :, at], out_s.at[3])
    done(pe.at[pl.ds(1, NZ - 1)], pz_r)
    total = pb[0]
    for dz in range(1, NZ):
        total = total + pe[dz]
    gg[...] = total[0:2] / gw[...]
    put(gg, gg_out, out_s.at[4])
    with jax.named_scope("gather"):
        done(gx.at[0, pl.ds(0, 3 * TOK)], t_r)
    with jax.named_scope("drain"):
        done(bk.at[pl.ds(0, count["z"] // 2)], z_s)
        done(rb.at[pl.ds(0, 7)], rb_s)
        done(sx.at[:, pl.ds(1, PLANE - 1)], ip_s)
        done(rq.at[pl.ds(0, 2), pl.ds(0, count["x"] // 2)], x_s)
        done(rq.at[0, 0], xf_s)
        done(wq, w_s)
        done(gx.at[pl.ds(0, 2)], g_s)
        done(gx.at[0], gf_s)
        done(prx, p_s)
        done(prs.at[pl.ds(1, PLANE - 1)], pp_s)
        done(pb.at[pl.ds(0, NZ - 1)], pz_s)
        done(igs.at[:, pl.ds(SLOT, ROWS - SLOT)], ig_s)
        done(db.at[pl.ds(0, 7)], c_s)
        done(gx.at[0, pl.ds(0, 3 * TOK)], t_s)
        done(tq, out_s.at[0])
        done(dg, out_s.at[1])
        done(du, out_s.at[2])
        done(dd, out_s.at[3])
        done(gg, out_s.at[4])


def carry(tg, gg, dg, du, dd, tg_out, gg_out, dg_out, du_out, dd_out, tg_v, gg_v, w_v, d_v, in_s, out_s):
    pairs = [(tg, tg_v, tg_out), (gg, gg_v, gg_out)]
    for i, (a, b) in enumerate(((dg, dg_out), (du, du_out), (dd, dd_out))):
        for k in range(2):
            pairs.append((a.at[k], w_v.at[2 * i + k] if i < 2 else d_v.at[k], b.at[k]))
    views = []
    for i, (a, v, b) in enumerate(pairs):
        views.append((pltpu.make_async_copy(a, v, in_s.at[i]), pltpu.make_async_copy(v, b, out_s.at[i])))
    for load, _ in views:
        load.start()
    for load, store in views:
        load.wait()
        store.start()
    for _, store in views:
        store.wait()


def shards(tokens, cotangent, routing, gate_weights, gate_proj, up_proj, down_proj):
    hbm = pl.BlockSpec(memory_space=pl.ANY)
    dma = pltpu.SemaphoreType.DMA
    scratch = [
        pltpu.VMEM((2, TOK), I32),
        pltpu.VMEM((2, TOK), F32),
        pltpu.VMEM((2, TOK), F32),
        pltpu.VMEM((len(HELD), 2, TOK, Q), BF16),
        pltpu.VMEM((NZ, 8, TOK), F32),
        pltpu.VMEM((len(BUILT), PLANE, 6, 8, Q), BF16),
        pltpu.VMEM((4, NZ, PLANE, 6, 8, Q), BF16),
        pltpu.VMEM((2, 2, D, FS), BF16),
        pltpu.VMEM((4, Q, 512), BF16),
        pltpu.VMEM((4, 256, Q), BF16),
        pltpu.VMEM((3, Q, 512), BF16),
        pltpu.VMEM((NZ, 8, TOK), I32),
        pltpu.VMEM((TOK, TOK), BF16),
        pltpu.VMEM((NZ, ROWS, TOK), BF16),
        pltpu.VMEM((NZ, ROWS, FS), F32),
        pltpu.VMEM((4, 2, ALL, Q), BF16),
        pltpu.VMEM((ALL, 512), BF16),
        pltpu.VMEM((ALL, 256), BF16),
        pltpu.VMEM((4, ALL, 256), BF16),
        pltpu.VMEM((2, PLANE, FS), F32),
        pltpu.VMEM((3, 2, PLANE, FS), F32),
        pltpu.VMEM((PLANE, 2, FS), F32),
        pltpu.VMEM((PLANE, 2, FS), F32),
        pltpu.VMEM((NZ, 8, Q), F32),
        pltpu.VMEM((NZ, 8, Q), F32),
        pltpu.VMEM((NZ, ROWS, Q), F32),
        pltpu.VMEM((NZ, ROWS, Q), F32),
        pltpu.VMEM((NZ, TOK, Q), F32),
        pltpu.VMEM((4, TOK, Q), F32),
        pltpu.VMEM((4, TOK, Q), F32),
        pltpu.VMEM((TOK, Q), BF16),
        pltpu.VMEM((2, D, FS), F32),
        pltpu.VMEM((2, D, FS), F32),
        pltpu.VMEM((2, FS, D), F32),
        dma((6,)), dma, dma((len(HELD), 2)), dma, dma((8,)),
        dma, dma((len(BUILT),)),
        dma, dma((2, 8)), dma, dma((2,)),
        dma, dma, dma, dma((2, 8)), dma, dma((8,)),
        dma, dma, dma, dma, dma, dma, dma, dma((8,)),
        dma, dma((4, 8)), dma, dma, dma((5,)),
    ]
    tg, gg, dg, du, dd = pl.pallas_call(
        kernel,
        out_shape=(
            jax.ShapeDtypeStruct((TOK, D), BF16),
            jax.ShapeDtypeStruct((2, TOK), F32),
            jax.ShapeDtypeStruct((2, D, FS), F32),
            jax.ShapeDtypeStruct((2, D, FS), F32),
            jax.ShapeDtypeStruct((2, FS, D), F32),
        ),
        in_specs=[hbm] * 7,
        out_specs=(hbm,) * 5,
        scratch_shapes=scratch,
        compiler_params=pltpu.CompilerParams(
            collective_id=0, has_side_effects=True, vmem_limit_bytes=63 * 1024 * 1024
        ),
    )(tokens, cotangent, routing.T, gate_weights.T, gate_proj, up_proj, down_proj)
    wide = jax.ShapeDtypeStruct((2, D, FS), F32)
    tg, gg, dg, du, dd = pl.pallas_call(
        carry,
        out_shape=(
            jax.ShapeDtypeStruct((TOK, D), BF16),
            jax.ShapeDtypeStruct((2, TOK), F32),
            wide, wide,
            jax.ShapeDtypeStruct((2, FS, D), F32),
        ),
        in_specs=[hbm] * 5,
        out_specs=(hbm,) * 5,
        scratch_shapes=[
            pltpu.VMEM((TOK, D), BF16),
            pltpu.VMEM((2, TOK), F32),
            pltpu.VMEM((4, D, FS), F32),
            pltpu.VMEM((2, FS, D), F32),
            dma((8,)),
            dma((8,)),
        ],
        compiler_params=pltpu.CompilerParams(vmem_limit_bytes=63 * 1024 * 1024),
    )(tg, gg, dg, du, dd)
    return tg, gg.T, dg, du, dd


def solution(mesh):
    in_specs = (
        P("ep", None),
        P("ep", None),
        P("ep", None),
        P("ep", None),
        P("ep", None, "tp"),
        P("ep", None, "tp"),
        P("ep", "tp", None),
    )
    out_specs = (
        P("ep", None),
        P("ep", None),
        P("ep", None, "tp"),
        P("ep", None, "tp"),
        P("ep", "tp", None),
    )
    return jax.shard_map(shards, mesh=mesh, in_specs=in_specs, out_specs=out_specs, check_vma=False)
```
